32 devices in a mesh: sp: 8 (over z, y), tp: 4 (over x, core).
Axes of the slice: x: 2, y: 2, z: 4, core: 2. Of those that a mesh axis runs over, the one named last changes fastest.
Arguments:
- residual: bfloat16 [5120, 2048], P(('sp', 'tp')), may hold values from -6 to 6
- small_value_inputs: bfloat16 [5120, 1024], P('sp', 'tp'), may hold values from -6 to 6
- large_value_inputs: bfloat16 [5120, 1024], P('sp', 'tp'), may hold values from -6 to 6
- small_gate_inputs: bfloat16 [5120, 1024], P('sp', 'tp'), may hold values from -6 to 6
- large_gate_inputs: bfloat16 [5120, 1024], P('sp', 'tp'), may hold values from -6 to 6
- state_projections: bfloat16 [5120, 4, 128], P('sp'), may hold values from -6 to 6
- small_step_inputs: bfloat16 [5120, 16], P('sp', 'tp'), may hold values from -2.5 to 2.5
- large_step_inputs: bfloat16 [5120, 8], P('sp', 'tp'), may hold values from -2.5 to 2.5
- small_decay_offsets: float32 [5120, 16], P('sp', 'tp'), may hold values from -1.4 to 0
- large_decay_offsets: float32 [5120, 8], P('sp', 'tp'), may hold values from -1.4 to 0
- small_decay_rates: float32 [16], P('tp'), may hold values from -11.1 to -3.1
- large_decay_rates: float32 [8], P('tp'), may hold values from -11.1 to -3.1
- small_filter_taps: bfloat16 [4, 1024], P(None, 'tp'), may hold values from -3 to 3
- large_filter_taps: bfloat16 [4, 1024], P(None, 'tp'), may hold values from -3 to 3
- state_filter_taps: bfloat16 [4, 4, 128], replicated, may hold values from -3 to 3
- small_head_gains: float32 [1024], P('tp'), may hold values from 0.1 to 1.9
- large_head_gains: float32 [1024], P('tp'), may hold values from 0.1 to 1.9
- small_output_projection: bfloat16 [1024, 2048], P('tp'), may hold values from -0.125 to 0.125
- large_output_projection: bfloat16 [1024, 2048], P('tp'), may hold values from -0.125 to 0.125
- channel_norm_gain: float32 [2048], replicated, may hold values from 0.1 to 1.9
- gate_matrix: bfloat16 [2048, 5632], P('sp', 'tp'), may hold values from -0.125 to 0.125
- up_matrix: bfloat16 [2048, 5632], P('sp', 'tp'), may hold values from -0.125 to 0.125
- down_matrix: bfloat16 [5632, 2048], P('tp', 'sp'), may hold values from -0.078125 to 0.078125
Outputs:
- layer_out: bfloat16 [5120, 2048], P(('sp', 'tp'))
The draws below stay inside these ranges and needn't reach their ends.
All inputs are finite; a program needn't handle non-finite values.
Results may differ from the reference program's by a relative error of at most 0.015.
Values may be sent and summed in bfloat16 or wider, within the bound.
No kernel may reach another device: no remote copies, remote signals or barrier semaphores. Data moves between devices by JAX's collectives and lax.ppermute only.
A program may use at most 64 MiB of HBM per device.

```python
import jax
import jax.numpy as jnp
from jax import lax

D = 2048
FF = 5632
SMALL_HEADS = 16
LARGE_HEADS = 8
STATE = 128
BLOCK = 64
CONV = 4
TOK_DEV = 640
TOKENS = 5120
W1 = 1024
W2 = 1024
N_TP = 4


def step_draw(key, head_outputs):
    first, second = jax.random.split(key)
    blocks = TOKENS // TOK_DEV
    offset = jax.random.uniform(first, (blocks, 1, head_outputs), jnp.float32, -1.0, 1.0)
    base = 0.5 * jax.random.truncated_normal(second, -3.0, 3.0, (blocks, TOK_DEV, head_outputs), jnp.float32)
    return (base + offset).reshape(TOKENS, head_outputs).astype(jnp.bfloat16)


def rate_draw(key, head_outputs):
    first, second, third = jax.random.split(key, 3)
    quick = jax.random.uniform(first, (head_outputs,), jnp.float32) < 0.5
    slow_rate = jax.random.uniform(second, (head_outputs,), jnp.float32, 0.2, 0.8) / (0.75 * TOKENS)
    fast_rate = 1.0 / (0.75 * jax.random.uniform(third, (head_outputs,), jnp.float32, 30.0, 100.0))
    return jnp.log(jnp.where(quick, fast_rate, slow_rate)).astype(jnp.float32)


def decay_offset_sample(key, head_outputs):
    first, second = jax.random.split(key)
    places = jax.random.randint(first, (2, head_outputs), 0, TOKENS)
    sizes = jnp.log(jax.random.uniform(second, (2, head_outputs), jnp.float32, 0.5, 0.8))
    hit = jnp.arange(TOKENS, dtype=jnp.int32)[:, None, None] == places[None, :, :]
    return jnp.sum(jnp.where(hit, sizes[None, :, :], 0.0), axis=1).astype(jnp.float32)


def draw_small_step_inputs(key, part):
    return step_draw(jax.random.fold_in(key, 11), SMALL_HEADS)


def draw_large_step_inputs(key, part):
    return step_draw(jax.random.fold_in(key, 12), LARGE_HEADS)


def draw_small_decay_rates(key, part):
    return rate_draw(jax.random.fold_in(key, 21), SMALL_HEADS)


def draw_large_decay_rates(key, part):
    return rate_draw(jax.random.fold_in(key, 22), LARGE_HEADS)


def draw_small_decay_offsets(key, part):
    return decay_offset_sample(jax.random.fold_in(key, 31), SMALL_HEADS)


def draw_large_decay_offsets(key, part):
    return decay_offset_sample(jax.random.fold_in(key, 32), LARGE_HEADS)


def steps_of(own_key, dims, cuts, low, largest):
    level = 1.0
    for position, blocks in cuts:
        heights = jax.random.uniform(jax.random.fold_in(jax.random.fold_in(own_key, 6), position), (blocks,), jnp.float32, low / len(cuts), largest / len(cuts))
        level = level * jnp.repeat(jnp.exp(heights), dims[position] // blocks).reshape((-1,) + (1,) * (len(dims) - 1 - position))
    return level


def normal_values(stream_key, shape, scale, bound, cuts=(), kind=jnp.bfloat16):
    result = jax.random.normal(stream_key, shape, jnp.float32) * scale
    if len(cuts) > 0:
        result = steps_of(stream_key, shape, cuts, -0.22, 0.18) * result
    return jnp.clip(result, min=-bound, max=bound).astype(kind)


def setup_inputs(seed: int = 0) -> dict:
    arg_keys = jax.random.split(jax.random.key(seed), 24)
    return {
        "residual": normal_values(arg_keys[0], (TOKENS, D), 1.0, 6.0, ((0, 32),)),
        "small_value_inputs": normal_values(arg_keys[1], (TOKENS, W1), 1.0, 6.0, ((0, 8), (1, 4))),
        "large_value_inputs": normal_values(arg_keys[2], (TOKENS, W2), 1.0, 6.0, ((0, 8), (1, 4))),
        "small_gate_inputs": normal_values(arg_keys[3], (TOKENS, W1), 1.0, 6.0, ((0, 8), (1, 4))),
        "large_gate_inputs": normal_values(arg_keys[4], (TOKENS, W2), 1.0, 6.0, ((0, 8), (1, 4))),
        "state_projections": normal_values(arg_keys[5], (TOKENS, 4, STATE), 1.0, 6.0, ((0, 8),)),
        "small_step_inputs": draw_small_step_inputs(jax.random.fold_in(arg_keys[23], 71), 0),
        "large_step_inputs": draw_large_step_inputs(jax.random.fold_in(arg_keys[23], 71), 0),
        "small_decay_offsets": draw_small_decay_offsets(jax.random.fold_in(arg_keys[23], 71), 0),
        "large_decay_offsets": draw_large_decay_offsets(jax.random.fold_in(arg_keys[23], 71), 0),
        "small_decay_rates": draw_small_decay_rates(jax.random.fold_in(arg_keys[23], 71), 0),
        "large_decay_rates": draw_large_decay_rates(jax.random.fold_in(arg_keys[23], 71), 0),
        "small_filter_taps": normal_values(arg_keys[12], (CONV, W1), CONV ** -0.5, 3.0, ((1, 4),)),
        "large_filter_taps": normal_values(arg_keys[13], (CONV, W2), CONV ** -0.5, 3.0, ((1, 4),)),
        "state_filter_taps": normal_values(arg_keys[14], (CONV, 4, STATE), CONV ** -0.5, 3.0),
        "small_head_gains": jnp.clip(1.0 + 0.18 * jax.random.normal(arg_keys[15], (W1,), jnp.float32), 0.1, 1.9),
        "large_head_gains": jnp.clip(1.0 + 0.18 * jax.random.normal(arg_keys[16], (W2,), jnp.float32), 0.1, 1.9),
        "small_output_projection": normal_values(arg_keys[17], (W1, D), (W1 + W2) ** -0.5, 0.125, ((0, 4),)),
        "large_output_projection": normal_values(arg_keys[18], (W2, D), (W1 + W2) ** -0.5, 0.125, ((0, 4),)),
        "channel_norm_gain": jnp.clip(1.0 + 0.18 * jax.random.normal(arg_keys[19], (D,), jnp.float32), 0.1, 1.9),
        "gate_matrix": normal_values(arg_keys[20], (D, FF), D ** -0.5, 0.125, ((0, 8), (1, 4))),
        "up_matrix": normal_values(arg_keys[21], (D, FF), D ** -0.5, 0.125, ((0, 8), (1, 4))),
        "down_matrix": normal_values(arg_keys[22], (FF, D), FF ** -0.5, 0.078125, ((0, 4), (1, 8))),
    }


HIGH = lax.Precision.HIGHEST
head_eps = 1e-05
row_eps = 1e-06

def rounded(value):
    return lax.optimization_barrier(value.astype(jnp.bfloat16)).astype(jnp.float32)

def causal_conv(series, prior_tokens, filter_taps):
    width = filter_taps.shape[0]
    length = series.shape[0]
    padded = jnp.concatenate([prior_tokens.astype(jnp.float32), series.astype(jnp.float32)], axis=0)
    total = jnp.zeros(series.shape, jnp.float32)
    for offset in range(width):
        total = total + filter_taps[offset].astype(jnp.float32)[None, :] * padded[offset:offset + length]
    return jax.nn.silu(total)

def block_scan(driven, decay_logarithm, key_vectors, read_vectors, state):
    length, head_outputs, size = driven.shape
    blocks = length // BLOCK
    mask = jnp.tril(jnp.ones((BLOCK, BLOCK), dtype=bool))[:, :, None]

    def advance(carry, pieces):
        values, decays, key_rows, read_rows = pieces
        within = jnp.cumsum(decays, axis=0)
        spread = within[:, None, :] - within[None, :, :]
        weights = jnp.where(mask, jnp.exp(jnp.where(mask, spread, 0.0)), 0.0)
        scores = jnp.dot(read_rows, key_rows.T, precision=HIGH)
        inner = jnp.einsum('ls,lsh,shp->lhp', scores, weights, values, precision=HIGH)
        carried = jnp.einsum('ln,hpn,lh->lhp', read_rows, carry, jnp.exp(within), precision=HIGH)
        tail = jnp.exp(within[-1][None, :] - within)
        fresh = jnp.einsum('ln,lh,lhp->hpn', key_rows, tail, values, precision=HIGH)
        return (carry * jnp.exp(within[-1])[:, None, None] + fresh, inner + carried)
    pieces = (driven.reshape(blocks, BLOCK, head_outputs, size), decay_logarithm.reshape(blocks, BLOCK, head_outputs), key_vectors.reshape(blocks, BLOCK, key_vectors.shape[1]), read_vectors.reshape(blocks, BLOCK, read_vectors.shape[1]))
    final, outs = lax.scan(advance, state, pieces)
    return (final, outs.reshape(length, head_outputs, size))

def heads_per_group(input_rows, gate_inputs, step_inputs, decay_offsets, decay_rates, filter_taps, head_gains, key_vectors, read_vectors):
    length, width = input_rows.shape
    head_outputs = decay_rates.shape[0]
    size = width // head_outputs
    prior_tokens = jnp.zeros((filter_taps.shape[0] - 1, width), jnp.bfloat16)
    conv_values = causal_conv(input_rows, prior_tokens, filter_taps)
    step_amount = jax.nn.softplus(step_inputs.astype(jnp.float32))
    decay_logarithm = -jnp.exp(decay_rates)[None, :] * step_amount + decay_offsets
    driven = conv_values.reshape(length, head_outputs, size) * step_amount[:, :, None]
    start_state = jnp.zeros((head_outputs, size, key_vectors.shape[1]), jnp.float32)
    _, scan_out = block_scan(driven, decay_logarithm, key_vectors, read_vectors, start_state)
    gated = scan_out * jax.nn.silu(gate_inputs.reshape(length, head_outputs, size).astype(jnp.float32))
    scale = lax.rsqrt(lax.optimization_barrier(jnp.mean(gated * gated, axis=-1, keepdims=True)) + head_eps)
    normed = gated * scale * head_gains.reshape(head_outputs, size).astype(jnp.float32)
    return normed.reshape(length, width).astype(jnp.bfloat16)

def row_norm(rows, gain):
    wide = rows.astype(jnp.float32)
    scale = lax.rsqrt(lax.optimization_barrier(jnp.mean(wide * wide, axis=-1, keepdims=True)) + row_eps)
    return (wide * scale * gain[None, :]).astype(jnp.bfloat16)

def reference(residual, small_value_inputs, large_value_inputs, small_gate_inputs, large_gate_inputs, state_projections, small_step_inputs, large_step_inputs, small_decay_offsets, large_decay_offsets, small_decay_rates, large_decay_rates, small_filter_taps, large_filter_taps, state_filter_taps, small_head_gains, large_head_gains, small_output_projection, large_output_projection, channel_norm_gain, gate_matrix, up_matrix, down_matrix):
    length = residual.shape[0]
    planes = state_projections.shape[1] * state_projections.shape[2]
    flat = state_projections.reshape(length, planes)
    flat_taps = state_filter_taps.reshape(state_filter_taps.shape[0], planes)
    prior_tokens = jnp.zeros((state_filter_taps.shape[0] - 1, planes), jnp.bfloat16)
    convolved_state_maps = causal_conv(flat, prior_tokens, flat_taps).reshape(length, state_projections.shape[1], state_projections.shape[2])
    small_head_outputs = heads_per_group(small_value_inputs, small_gate_inputs, small_step_inputs, small_decay_offsets, small_decay_rates, small_filter_taps, small_head_gains, convolved_state_maps[:, 0], convolved_state_maps[:, 1])
    large_head_outputs = heads_per_group(large_value_inputs, large_gate_inputs, large_step_inputs, large_decay_offsets, large_decay_rates, large_filter_taps, large_head_gains, convolved_state_maps[:, 2], convolved_state_maps[:, 3])
    slice_small = W1 // N_TP
    slice_large = W2 // N_TP
    mixed = jnp.zeros((length, D), jnp.float32)
    for part in range(N_TP):
        term = jnp.dot(small_head_outputs[:, part * slice_small:(part + 1) * slice_small], small_output_projection[part * slice_small:(part + 1) * slice_small], preferred_element_type=jnp.float32)
        term = term + jnp.dot(large_head_outputs[:, part * slice_large:(part + 1) * slice_large], large_output_projection[part * slice_large:(part + 1) * slice_large], preferred_element_type=jnp.float32)
        mixed = mixed + rounded(term)
    middle = (residual.astype(jnp.float32) + mixed).astype(jnp.bfloat16)
    normed = row_norm(middle, channel_norm_gain)
    gate = jnp.dot(normed, gate_matrix, preferred_element_type=jnp.float32)
    up = jnp.dot(normed, up_matrix, preferred_element_type=jnp.float32)
    hidden = (jax.nn.silu(gate) * up).astype(jnp.bfloat16)
    slice_units = FF // N_TP
    down = jnp.zeros((length, D), jnp.float32)
    for part in range(N_TP):
        down = down + rounded(jnp.dot(hidden[:, part * slice_units:(part + 1) * slice_units], down_matrix[part * slice_units:(part + 1) * slice_units], preferred_element_type=jnp.float32))
    return (middle.astype(jnp.float32) + down).astype(jnp.bfloat16)
```

```python
import functools

import jax
import jax.numpy as jnp
from jax import lax
from jax.experimental import pallas as pl
from jax.experimental.pallas import tpu as pltpu
from jax.sharding import PartitionSpec as P

HIGH = lax.Precision.HIGHEST
HEAD_EPS = 1e-05
ROW_EPS = 1e-06
HALO = 8
EXTRA = 16
AXES = ("sp", "tp")


f32 = jnp.float32
bf16 = jnp.bfloat16
VMEM = pl.BlockSpec(memory_space=pltpu.VMEM)
SMEM = pl.BlockSpec(memory_space=pltpu.SMEM)
ANY = pl.BlockSpec(memory_space=pl.ANY)


def block_of(length):
    for size in (128, 64, 32, 16, 8):
        if length % size == 0:
            return size
    return length


def dot(a, b, precision=None):
    return jnp.dot(a, b, preferred_element_type=f32, precision=precision)


def dot_first(a, b):
    return lax.dot_general(a, b, (((0,), (0,)), ((), ())), preferred_element_type=f32)


def one_hot(heads, width):
    size = width // heads
    head = lax.broadcasted_iota(jnp.int32, (heads, width), 0)
    channel = lax.broadcasted_iota(jnp.int32, (heads, width), 1)
    return jnp.where((channel >= head * size) & (channel < (head + 1) * size), 1.0, 0.0).astype(f32)


def spread(per_head, hot):
    return dot(per_head, hot, HIGH)


def conv(pad_ref, halo, series, taps):
    length, width = series.shape
    pad_ref[0:HALO, 0:width] = halo.astype(f32)
    pad_ref[HALO : HALO + length, 0:width] = series.astype(f32)
    count = taps.shape[0]
    total = jnp.zeros((length, width), f32)
    for k in range(count):
        first = HALO - (count - 1) + k
        total = total + taps[k : k + 1, :].astype(f32) * pad_ref[first : first + length, 0:width]
    return total * (1.0 / (1.0 + jnp.exp(-total)))


def softplus(x):
    return jnp.maximum(x, 0.0) + jnp.log1p(jnp.exp(-jnp.abs(x)))


def start_kernel(widths, heads, state, halo_ref, vs_ref, vl_ref, flat_ref, ss_ref, sl_ref, os_ref, ol_ref, rs_ref, rl_ref,
                 ts_ref, tl_ref, tm_ref, driven_ref, maps_ref, cs_ref, cl_ref, msg_ref, pad_ref):
    length = vs_ref.shape[0]
    size = block_of(length)
    offset = 0
    for plane in range(4):
        lo = plane * state
        hi = lo + state
        base = widths[0] + widths[1] + lo
        plane_conv = conv(pad_ref, halo_ref[:, base : base + state], flat_ref[:, lo:hi], tm_ref[:, lo:hi])
        maps_ref[:, lo:hi] = plane_conv.astype(bf16)
    row = lax.broadcasted_iota(jnp.int32, (size, size), 0)
    col = lax.broadcasted_iota(jnp.int32, (size, size), 1)
    tri = jnp.where(row >= col, 1.0, 0.0).astype(f32)
    kinds = ((vs_ref, ss_ref, os_ref, rs_ref, ts_ref, cs_ref), (vl_ref, sl_ref, ol_ref, rl_ref, tl_ref, cl_ref))
    for kind, (v_ref, s_ref, o_ref, r_ref, t_ref, c_ref) in enumerate(kinds):
        width = widths[kind]
        hot = one_hot(heads[kind], width)
        step = softplus(s_ref[...].astype(f32))
        log_decay = -jnp.exp(r_ref[...]) * step + o_ref[...]
        base = jnp.zeros((1, heads[kind]), f32)
        for i in range(length // size):
            within = dot(tri, log_decay[i * size : (i + 1) * size], HIGH)
            c_ref[i * size : (i + 1) * size, :] = within + base
            base = base + within[size - 1 : size]
        values = conv(pad_ref, halo_ref[:, offset : offset + width], v_ref[...], t_ref[...])
        driven = values * spread(step, hot)
        driven_ref[:, offset : offset + width] = driven.astype(bf16)
        tail = jnp.exp(base - c_ref[...])
        fresh = (driven * spread(tail, hot)).astype(bf16)
        keys = maps_ref[:, 2 * kind * state : (2 * kind + 1) * state]
        final = dot_first(keys, fresh)
        msg_ref[0:state, offset : offset + width] = final.astype(bf16)
        total = spread(jnp.exp(base), hot)
        high = total.astype(bf16)
        low = (total - high.astype(f32)).astype(bf16)
        place = lax.broadcasted_iota(jnp.int32, (EXTRA, width), 0)
        rows = jnp.where(place == 0, high.astype(f32), jnp.where(place == 1, low.astype(f32), 0.0))
        msg_ref[state : state + EXTRA, offset : offset + width] = rows.astype(bf16)
        offset += width


def local_kernel(widths, heads, state, driven_ref, maps_ref, cs_ref, cl_ref, out_ref):
    length = driven_ref.shape[0]
    size = block_of(length)
    row = lax.broadcasted_iota(jnp.int32, (size, size), 0)
    col = lax.broadcasted_iota(jnp.int32, (size, size), 1)
    mask = row >= col
    offset = 0
    for kind, c_ref in enumerate((cs_ref, cl_ref)):
        width = widths[kind]
        count = heads[kind]
        each = width // count
        hot = one_hot(count, width)
        carry = jnp.zeros((state, width), f32)
        base = jnp.zeros((1, count), f32)
        for i in range(length // size):
            here = slice(i * size, (i + 1) * size)
            keys = maps_ref[here, 2 * kind * state : (2 * kind + 1) * state]
            reads = maps_ref[here, (2 * kind + 1) * state : (2 * kind + 2) * state]
            driven = driven_ref[here, offset : offset + width]
            within = c_ref[here, :] - base
            across = within.T
            last = within[size - 1 : size]
            scores = lax.dot_general(reads, keys, (((1,), (1,)), ((), ())), preferred_element_type=f32)
            parts = []
            for h in range(count):
                gap = within[:, h : h + 1] - across[h : h + 1, :]
                weights = jnp.where(mask, jnp.exp(jnp.where(mask, gap, 0.0)), 0.0)
                parts.append(dot((scores * weights).astype(bf16), driven[:, h * each : (h + 1) * each]))
            inner = jnp.concatenate(parts, axis=1)
            if i > 0:
                inner = inner + dot(reads, carry.astype(bf16)) * spread(jnp.exp(within), hot)
            out_ref[here, offset : offset + width] = inner
            if i + 1 < length // size:
                fresh = (driven.astype(f32) * spread(jnp.exp(last - within), hot)).astype(bf16)
                carry = carry * spread(jnp.exp(last), hot) + dot_first(keys, fresh)
            base = base + last
        offset += width


def decay_of(ref, state):
    return ref[state : state + 1, :].astype(f32) + ref[state + 1 : state + 2, :].astype(f32)


def group_kernel(group, state, place_ref, *refs):
    out_ref, before_ref = refs[group], refs[group + 1]
    place = place_ref[0]
    places = [lax.rem(place - k + group, group) for k in range(group)]
    decays = [decay_of(ref, state) for ref in refs[:group]]
    ones = jnp.ones_like(decays[0])
    total = jnp.zeros((state, ones.shape[1]), f32)
    before = jnp.zeros_like(total)
    total_decay = ones
    before_decay = ones
    for k in range(group):
        rest = ones
        rest_before = ones
        for m in range(group):
            if m != k:
                rest = jnp.where(places[m] > places[k], rest * decays[m], rest)
                rest_before = jnp.where((places[m] > places[k]) & (places[m] < place), rest_before * decays[m], rest_before)
        values = refs[k][0:state, :].astype(f32)
        total = total + values * rest
        total_decay = total_decay * decays[k]
        if k > 0:
            is_before = places[k] < place
            before = before + jnp.where(is_before, values * rest_before, 0.0)
            before_decay = jnp.where(is_before, before_decay * decays[k], before_decay)
    index = lax.broadcasted_iota(jnp.int32, (EXTRA, ones.shape[1]), 0)
    for ref, values, decay in ((out_ref, total, total_decay), (before_ref, before, before_decay)):
        ref[0:state, :] = values.astype(bf16)
        high = decay.astype(bf16).astype(f32)
        rows = jnp.where(index == 0, high, jnp.where(index == 1, decay - high, 0.0))
        ref[state : state + EXTRA, :] = rows.astype(bf16)


def finish_kernel(widths, heads, state, ways, hops, place_ref, local_ref, maps_ref, cs_ref, cl_ref, gs_ref, gl_ref, hs_ref,
                  hl_ref, ws_ref, wl_ref, before_ref, *refs):
    arrived = refs[:hops]
    keep_ref, send_ref, rows_ref = refs[hops:]
    length = local_ref.shape[0]
    per = length // ways
    incoming = jnp.zeros((state, local_ref.shape[1]), f32)
    for ref in reversed(arrived):
        incoming = ref[0:state, :].astype(f32) + decay_of(ref, state) * incoming
    incoming = incoming * decay_of(before_ref, state) + before_ref[0:state, :].astype(f32)
    incoming = incoming.astype(bf16)
    offset = 0
    kinds = ((cs_ref, gs_ref, hs_ref), (cl_ref, gl_ref, hl_ref))
    for kind, (c_ref, g_ref, h_ref) in enumerate(kinds):
        width = widths[kind]
        count = heads[kind]
        hot = one_hot(count, width)
        for i in range(ways):
            here = slice(i * per, (i + 1) * per)
            reads = maps_ref[here, (2 * kind + 1) * state : (2 * kind + 2) * state]
            scan = local_ref[here, offset : offset + width]
            scan = scan + dot(reads, incoming[:, offset : offset + width]) * spread(jnp.exp(c_ref[here, :]), hot)
            gates = g_ref[here, :].astype(f32)
            gated = scan * (gates / (1.0 + jnp.exp(-gates)))
            mean = lax.dot_general(gated * gated, hot, (((1,), (1,)), ((), ())), preferred_element_type=f32, precision=HIGH)
            scale = lax.rsqrt(mean * (count / width) + HEAD_EPS)
            normed = gated * spread(scale, hot) * h_ref[...]
            rows_ref[i, :, offset : offset + width] = normed.astype(bf16)
        offset += width
    place = place_ref[0]
    half = ways // 2
    for slot in range(half):
        for bit, ref in ((1, send_ref), (0, keep_ref)):
            rows = rows_ref[jnp.bitwise_xor(place, 2 * slot + bit)]
            part = dot(rows[:, : widths[0]], ws_ref[...]) + dot(rows[:, widths[0] :], wl_ref[...])
            ref[slot] = part.astype(bf16)


def norm_kernel(blocks, residual_ref, own_ref, other_ref, gain_ref, middle_ref, normed_ref):
    middle = residual_ref[...].astype(f32) + (own_ref[...].astype(f32) + other_ref[...].astype(f32))
    middle = middle.astype(bf16)
    middle_ref[...] = middle
    wide = middle.astype(f32)
    scale = lax.rsqrt(jnp.mean(wide * wide, axis=-1, keepdims=True) + ROW_EPS)
    normed = (wide * scale * gain_ref[...]).astype(bf16)
    width = normed.shape[1] // blocks
    for b in range(blocks):
        normed_ref[b] = normed[:, b * width : (b + 1) * width]


def channel_kernel(blocks, index_ref, rows_ref, *refs):
    gates, ups, downs = refs[:blocks], refs[blocks : 2 * blocks], refs[2 * blocks : 3 * blocks]
    out_ref, gate_ref, up_ref, down_ref, cat_ref, sems = refs[3 * blocks :]
    depth = gates[0].shape[0]

    def copies(kind):
        source = (gates, ups, downs)[kind]
        out = []
        for b in range(blocks):
            if kind < 2:
                target = (gate_ref, up_ref)[kind].at[pl.ds(b * depth, depth), :]
            else:
                target = down_ref.at[b]
            out.append(pltpu.make_async_copy(source[b], target, sems.at[kind, b]))
        return out

    started = [copies(kind) for kind in range(3)]
    for group in started:
        for copy in group:
            copy.start()
    for b in range(blocks):
        cat_ref[:, b * depth : (b + 1) * depth] = rows_ref[index_ref[b]]
    for copy in started[0]:
        copy.wait()
    gate = dot(cat_ref[...], gate_ref[...])
    gate = gate * (1.0 / (1.0 + jnp.exp(-gate)))
    for copy in started[1]:
        copy.wait()
    hidden = (gate * dot(cat_ref[...], up_ref[...])).astype(bf16)
    for b in range(blocks):
        started[2][b].wait()
        out_ref[index_ref[b]] = dot(hidden, down_ref[b]).astype(bf16)


def params(mib):
    return pltpu.CompilerParams(vmem_limit_bytes=mib * 1024 * 1024)


def cost(flops, nbytes):
    return pl.CostEstimate(flops=int(flops), bytes_accessed=int(nbytes), transcendentals=0)


def on_device(sizes, residual, small_values, large_values, small_gates, large_gates, state_projections, small_steps, large_steps,
              small_offsets, large_offsets, small_rates, large_rates, small_taps, large_taps, state_taps, small_gains, large_gains,
              small_projection, large_projection, norm_gain, gate_matrix, up_matrix, down_matrix):
    n_sp, n_tp = sizes
    n_f = n_tp
    n_g = n_sp // n_f
    n_x = n_tp // 2
    sp = lax.axis_index("sp")
    tp = lax.axis_index("tp")
    g = lax.rem(sp, n_g)

    def send(x, to):
        pairs = []
        for s in range(n_sp):
            for t in range(n_tp):
                target = to(s // n_g, s % n_g, t)
                if target is not None:
                    pairs.append((s * n_tp + t, (target[0] * n_g + target[1]) * n_tp + target[2]))
        return lax.ppermute(x, AXES, pairs)

    length, width_small = small_values.shape
    width_large = large_values.shape[1]
    widths = (width_small, width_large)
    width = width_small + width_large
    heads = (small_rates.shape[0], large_rates.shape[0])
    planes, state = state_projections.shape[1:]
    rows, model = residual.shape

    flat = state_projections.reshape(length, planes * state)
    edge = jnp.concatenate([small_values[length - HALO :], large_values[length - HALO :], flat[length - HALO :]], axis=1)
    halo = lax.ppermute(edge, "sp", [(i, i + 1) for i in range(n_sp - 1)])

    def gathered(matrix, order):
        first = send(matrix, lambda f_, g_, t_: (t_, g_, 2 * (f_ % n_x) + f_ // n_x))
        held = [(first, (0, 0, 0))]
        for kind in order:
            count = (n_x, n_g, 2)[kind]
            new = []
            for k in range(1, count):
                for block, way in held:
                    if kind == 0:
                        got = send(block, lambda f_, g_, t_: (f_, g_, 2 * ((t_ // 2 + k) % n_x) + t_ % 2))
                    elif kind == 1:
                        got = send(block, lambda f_, g_, t_: (f_, (g_ + k) % n_g, t_))
                    else:
                        got = send(block, lambda f_, g_, t_: (f_, g_, t_ ^ 1))
                    moved = list(way)
                    moved[kind] += k
                    new.append((got, tuple(moved)))
            held = held + new
        held.sort(key=lambda item: item[1])
        return [block for block, _ in held], [way for _, way in held]

    gates, ways = gathered(gate_matrix, (0, 1, 2))
    ups, _ = gathered(up_matrix, (1, 0, 2))
    downs, _ = gathered(down_matrix, (0, 1, 2))
    places = []
    for dx, dg, dc in ways:
        x_ = lax.rem(tp // 2 - dx + n_x, n_x)
        c_ = lax.rem(lax.rem(tp, 2) - dc + 2, 2)
        g_ = lax.rem(g - dg + n_g, n_g)
        places.append((c_ * n_x + x_) * n_g + g_)
    index = jnp.stack(places).astype(jnp.int32)
    blocks = n_sp

    message = jax.ShapeDtypeStruct((state + EXTRA, width), bf16)
    driven, maps, small_cum, large_cum, own = pl.pallas_call(
        functools.partial(start_kernel, widths, heads, state),
        out_shape=(
            jax.ShapeDtypeStruct((length, width), bf16),
            jax.ShapeDtypeStruct((length, planes * state), bf16),
            jax.ShapeDtypeStruct((length, heads[0]), f32),
            jax.ShapeDtypeStruct((length, heads[1]), f32),
            message,
        ),
        in_specs=[VMEM] * 13,
        out_specs=(VMEM,) * 5,
        scratch_shapes=[pltpu.VMEM((HALO + length, max(widths + (state,))), f32)],
        compiler_params=params(24),
        cost_estimate=cost(4e9, 4e6),
        name="start",
    )(halo, small_values, large_values, flat, small_steps, large_steps, small_offsets, large_offsets, small_rates[None, :],
      large_rates[None, :], small_taps, large_taps, state_taps.reshape(state_taps.shape[0], planes * state))

    others = [send(own, lambda f_, g_, t_: (f_, (g_ + k) % n_g, t_)) for k in range(1, n_g)]
    local = pl.pallas_call(
        functools.partial(local_kernel, widths, heads, state),
        out_shape=jax.ShapeDtypeStruct((length, width), f32),
        in_specs=[VMEM] * 4,
        out_specs=VMEM,
        compiler_params=params(24),
        cost_estimate=cost(6e9, 4e6),
        name="local",
    )(driven, maps, small_cum, large_cum)
    joined, before = pl.pallas_call(
        functools.partial(group_kernel, n_g, state),
        out_shape=(message, message),
        in_specs=[SMEM] + [VMEM] * n_g,
        out_specs=(VMEM, VMEM),
        compiler_params=params(16),
        cost_estimate=cost(1e9, 5e5),
        name="group",
    )(g[None].astype(jnp.int32), own, *others)
    arrived = [send(joined, lambda f_, g_, t_: (f_ + k, g_, t_) if f_ + k < n_f else None) for k in range(1, n_f)]

    half = n_tp // 2
    part = jax.ShapeDtypeStruct((half, rows, model), bf16)
    keep, give = pl.pallas_call(
        functools.partial(finish_kernel, widths, heads, state, n_tp, len(arrived)),
        out_shape=(part, part),
        in_specs=[SMEM] + [VMEM] * (11 + len(arrived)),
        out_specs=(VMEM, VMEM),
        scratch_shapes=[pltpu.VMEM((n_tp, rows, width), bf16)],
        compiler_params=params(32),
        cost_estimate=cost(6e9, 6e6),
        name="finish",
    )(tp[None].astype(jnp.int32), local, maps, small_cum, large_cum, small_gates, large_gates, small_gains[None, :],
      large_gains[None, :], small_projection, large_projection, before, *arrived)

    got = send(give, lambda f_, g_, t_: (f_, g_, t_ ^ 1))
    kept = [keep[i] for i in range(half)]
    arriving = [got[i] for i in range(half)]
    bit = 2
    while len(kept) > 1:
        sent = []
        stay = []
        for i in range(0, len(kept), 2):
            stay.append((kept[i].astype(f32) + arriving[i].astype(f32)).astype(bf16))
            sent.append((kept[i + 1].astype(f32) + arriving[i + 1].astype(f32)).astype(bf16))
        arriving = [send(x, lambda f_, g_, t_, b=bit: (f_, g_, t_ ^ b)) for x in sent]
        kept = stay
        bit *= 2
    middle, normed = pl.pallas_call(
        functools.partial(norm_kernel, blocks),
        out_shape=(
            jax.ShapeDtypeStruct((rows, model), bf16),
            jax.ShapeDtypeStruct((blocks, rows, model // blocks), bf16),
        ),
        in_specs=[VMEM] * 4,
        out_specs=(VMEM, VMEM),
        compiler_params=params(16),
        cost_estimate=cost(1e9, 3e6),
        name="norm",
    )(residual, kept[0], arriving[0], norm_gain[None, :])

    depth, hidden = gate_matrix.shape
    channel = pl.pallas_call(
        functools.partial(channel_kernel, blocks),
        out_shape=jax.ShapeDtypeStruct((blocks, rows, depth), bf16),
        in_specs=[SMEM, VMEM] + [ANY] * (3 * blocks),
        out_specs=VMEM,
        scratch_shapes=[
            pltpu.VMEM((model, hidden), bf16),
            pltpu.VMEM((model, hidden), bf16),
            pltpu.VMEM((blocks, hidden, depth), bf16),
            pltpu.VMEM((rows, model), bf16),
            pltpu.SemaphoreType.DMA((3, blocks)),
        ],
        compiler_params=params(40),
        cost_estimate=cost(6 * rows * model * hidden, 18e6),
        name="channel",
    )

    def ring(x):
        return send(x, lambda f_, g_, t_: ((f_ + 1) % n_f, g_, t_))

    chunks = [normed]
    for _ in range(1, n_f):
        chunks.append(ring(chunks[-1]))
    weights = (*gates, *ups, *downs)
    outs = [channel(index, chunk, *weights) for chunk in chunks]
    total = outs[1]
    for s in range(2, n_f):
        total = (ring(total).astype(f32) + outs[s].astype(f32)).astype(bf16)
    down = ring(total).astype(f32) + outs[0].astype(f32)
    down = down.transpose(1, 0, 2).reshape(rows, model)
    return (middle.astype(f32) + down).astype(bf16)


def solution(mesh):
    sizes = (mesh.shape["sp"], mesh.shape["tp"])
    in_specs = (
        P(AXES, None),
        P("sp", "tp"), P("sp", "tp"), P("sp", "tp"), P("sp", "tp"),
        P("sp", None, None),
        P("sp", "tp"), P("sp", "tp"), P("sp", "tp"), P("sp", "tp"),
        P("tp"), P("tp"),
        P(None, "tp"), P(None, "tp"),
        P(),
        P("tp"), P("tp"),
        P("tp", None), P("tp", None),
        P(),
        P("sp", "tp"), P("sp", "tp"), P("tp", "sp"),
    )
    return jax.shard_map(
        functools.partial(on_device, sizes), mesh=mesh, in_specs=in_specs, out_specs=P(AXES, None), check_vma=False
    )
```

```python
import functools

import jax
import jax.numpy as jnp
from jax import lax
from jax.experimental import pallas as pl
from jax.experimental.pallas import tpu as pltpu
from jax.sharding import PartitionSpec as P


HIGH = lax.Precision.HIGHEST
HEAD_EPS = 1e-05
ROW_EPS = 1e-06
HALO = 8
EXTRA = 16
AXES = ("sp", "tp")


f32 = jnp.float32
bf16 = jnp.bfloat16
VMEM = pl.BlockSpec(memory_space=pltpu.VMEM)
SMEM = pl.BlockSpec(memory_space=pltpu.SMEM)
HBM = pl.BlockSpec(memory_space=pltpu.HBM)


def block_of(length):
    for size in (128, 64, 32, 16, 8):
        if length % size == 0:
            return size
    return length


def dot(a, b, precision=None):
    return jnp.dot(a, b, preferred_element_type=f32, precision=precision)


def dot_first(a, b, precision=None):
    return lax.dot_general(a, b, (((0,), (0,)), ((), ())), preferred_element_type=f32, precision=precision)


def dot_last(a, b, precision=None):
    return lax.dot_general(a, b, (((1,), (1,)), ((), ())), preferred_element_type=f32, precision=precision)


def one_hot(heads, widths, mean=False):
    count = padded(sum(heads))
    total = sum(widths)
    head = lax.broadcasted_iota(jnp.int32, (count, total), 0)
    channel = lax.broadcasted_iota(jnp.int32, (count, total), 1)
    hot = jnp.zeros((count, total), f32)
    first, start = 0, 0
    for number, width in zip(heads, widths):
        size = width // number
        low = start + (head - first) * size
        inside = (head >= first) & (head < first + number) & (channel >= low) & (channel < low + size)
        hot = jnp.where(inside, 1.0 / size if mean else 1.0, hot)
        first += number
        start += width
    return hot


def padded(count):
    return -(-count // 8) * 8


def silu(x):
    return x * (1.0 / (1.0 + jnp.exp(-x)))


def conv(pad_ref, halo, series, taps):
    length, width = series.shape
    pad_ref[0:HALO, 0:width] = halo.astype(f32)
    pad_ref[HALO : HALO + length, 0:width] = series.astype(f32)
    total = jnp.zeros((length, width), f32)
    for k, tap in enumerate(taps):
        first = HALO - (len(taps) - 1) + k
        total = total + tap.astype(f32) * pad_ref[first : first + length, 0:width]
    return silu(total)


def softplus(x):
    return jnp.maximum(x, 0.0) + jnp.log1p(jnp.exp(-jnp.abs(x)))


def edge_kernel(state, vs_ref, vl_ref, proj_ref, out_ref):
    first = vs_ref.shape[1]
    second = first + vl_ref.shape[1]
    out_ref[:, :first] = vs_ref[...]
    out_ref[:, first:second] = vl_ref[...]
    for plane in range(proj_ref.shape[1]):
        lo = second + plane * state
        out_ref[:, lo : lo + state] = proj_ref[:, plane, :]


def start_kernel(widths, heads, state, rs_ref, rl_ref, halo_ref, vs_ref, vl_ref, proj_ref, ss_ref, sl_ref, os_ref, ol_ref,
                 ts_ref, tl_ref, tm_ref, driven_ref, maps_ref, cum_ref, msg_ref, pad_ref, step_ref):
    length = vs_ref.shape[0]
    size = block_of(length)
    step_ref[...] = jnp.zeros_like(step_ref)
    cum_ref[...] = jnp.zeros_like(cum_ref)
    first = 0
    for number, s_ref, o_ref, r_ref in ((heads[0], ss_ref, os_ref, rs_ref), (heads[1], sl_ref, ol_ref, rl_ref)):
        step = softplus(s_ref[...].astype(f32))
        step_ref[first : first + number, :] = step
        for h in range(number):
            rate = jnp.exp(jnp.full((1, length), r_ref[h], f32))
            cum_ref[first + h : first + h + 1, :] = o_ref[h : h + 1, :] - rate * step[h : h + 1, :]
        first += number
    row = lax.broadcasted_iota(jnp.int32, (size, size), 0)
    col = lax.broadcasted_iota(jnp.int32, (size, size), 1)
    tri = jnp.where(row <= col, 1.0, 0.0).astype(f32)
    base = jnp.zeros((cum_ref.shape[0], 1), f32)
    for i in range(length // size):
        within = dot(cum_ref[:, i * size : (i + 1) * size], tri, HIGH) + base
        cum_ref[:, i * size : (i + 1) * size] = within
        base = within[:, size - 1 : size]
    hot = one_hot(heads, widths)
    count = tm_ref.shape[0]
    for plane in range(4):
        lo = plane * state
        at = sum(widths) + lo
        taps = [tm_ref[k, plane : plane + 1, :] for k in range(count)]
        done = conv(pad_ref, halo_ref[:, at : at + state], proj_ref[:, plane, :], taps)
        maps_ref[:, lo : lo + state] = done.astype(bf16)
    steps = dot_first(step_ref[...], hot, HIGH)
    tails = dot_first(jnp.exp(base - cum_ref[...]), hot, HIGH)
    offset = 0
    for kind, (width, v_ref, t_ref) in enumerate(((widths[0], vs_ref, ts_ref), (widths[1], vl_ref, tl_ref))):
        there = slice(offset, offset + width)
        taps = [t_ref[k : k + 1, :] for k in range(count)]
        driven = conv(pad_ref, halo_ref[:, there], v_ref[...], taps) * steps[:, there]
        driven_ref[:, there] = driven.astype(bf16)
        keys = maps_ref[:, 2 * kind * state : (2 * kind + 1) * state]
        msg_ref[0:state, there] = dot_first(keys, (driven * tails[:, there]).astype(bf16)).astype(bf16)
        offset += width
    write_decay(msg_ref, state, dot_first(jnp.exp(base), hot, HIGH))


def write_decay(ref, state, decay):
    high = decay.astype(bf16).astype(f32)
    index = lax.broadcasted_iota(jnp.int32, (EXTRA, decay.shape[1]), 0)
    rows = jnp.where(index == 0, high, jnp.where(index == 1, decay - high, 0.0))
    ref[state : state + EXTRA, :] = rows.astype(bf16)


def decay_of(ref, state):
    return ref[state : state + 1, :].astype(f32) + ref[state + 1 : state + 2, :].astype(f32)


def local_kernel(widths, heads, state, driven_ref, maps_ref, cum_ref, out_ref):
    length = driven_ref.shape[0]
    size = block_of(length)
    row = lax.broadcasted_iota(jnp.int32, (size, size), 0)
    col = lax.broadcasted_iota(jnp.int32, (size, size), 1)
    mask = row >= col
    hot = one_hot(heads, widths)
    base = jnp.zeros((cum_ref.shape[0], 1), f32)
    carry = [jnp.zeros((state, width), f32) for width in widths]
    for i in range(length // size):
        here = slice(i * size, (i + 1) * size)
        within = cum_ref[:, here] - base
        down = within.T
        last = within[:, size - 1 : size]
        grown = dot_first(jnp.exp(within), hot, HIGH)
        tails = dot_first(jnp.exp(last - within), hot, HIGH)
        whole = grown[size - 1 : size, :]
        base = base + last
        offset, first = 0, 0
        for kind in range(2):
            width, number = widths[kind], heads[kind]
            each = width // number
            there = slice(offset, offset + width)
            keys = maps_ref[here, 2 * kind * state : (2 * kind + 1) * state]
            reads = maps_ref[here, (2 * kind + 1) * state : (2 * kind + 2) * state]
            driven = driven_ref[here, there]
            scores = dot_last(reads, keys)
            parts = []
            for h in range(number):
                gap = down[:, first + h : first + h + 1] - within[first + h : first + h + 1, :]
                weights = jnp.where(mask, jnp.exp(jnp.where(mask, gap, 0.0)), 0.0)
                parts.append(dot((scores * weights).astype(bf16), driven[:, h * each : (h + 1) * each]))
            inner = jnp.concatenate(parts, axis=1) if number > 1 else parts[0]
            if i > 0:
                inner = inner + dot(reads, carry[kind].astype(bf16)) * grown[:, there]
            out_ref[here, there] = inner
            if i + 1 < length // size:
                fresh = (driven.astype(f32) * tails[:, there]).astype(bf16)
                carry[kind] = carry[kind] * whole[:, there] + dot_first(keys, fresh)
            offset += width
            first += number


def group_kernel(group, state, place_ref, *refs):
    out_ref, before_ref = refs[group], refs[group + 1]
    place = place_ref[0]
    places = [lax.rem(place - k + group, group) for k in range(group)]
    decays = [decay_of(ref, state) for ref in refs[:group]]
    ones = jnp.ones_like(decays[0])
    total = jnp.zeros((state, ones.shape[1]), f32)
    before = jnp.zeros_like(total)
    total_decay = ones
    before_decay = ones
    for k in range(group):
        rest = ones
        rest_before = ones
        for m in range(group):
            if m != k:
                rest = jnp.where(places[m] > places[k], rest * decays[m], rest)
                rest_before = jnp.where((places[m] > places[k]) & (places[m] < place), rest_before * decays[m], rest_before)
        values = refs[k][0:state, :].astype(f32)
        total = total + values * rest
        total_decay = total_decay * decays[k]
        if k > 0:
            is_before = places[k] < place
            before = before + jnp.where(is_before, values * rest_before, 0.0)
            before_decay = jnp.where(is_before, before_decay * decays[k], before_decay)
    for ref, values, decay in ((out_ref, total, total_decay), (before_ref, before, before_decay)):
        ref[0:state, :] = values.astype(bf16)
        write_decay(ref, state, decay)


def finish_kernel(widths, heads, state, ways, hops, place_ref, gs_far, gl_far, ws_far, wl_far, local_ref, maps_ref, cum_ref,
                  hs_ref, hl_ref, before_ref, *refs):
    arrived = refs[:hops]
    keep_ref, send_ref, rows_ref, gs_ref, gl_ref, ws_ref, wl_ref, sems = refs[hops:]
    pairs = ((gs_far, gs_ref), (gl_far, gl_ref), (ws_far, ws_ref), (wl_far, wl_ref))
    copies = [pltpu.make_async_copy(far, near, sems.at[k]) for k, (far, near) in enumerate(pairs)]
    for copy in copies:
        copy.start()
    length = local_ref.shape[0]
    size = block_of(length)
    incoming = jnp.zeros((state, local_ref.shape[1]), f32)
    for ref in reversed(arrived):
        incoming = ref[0:state, :].astype(f32) + decay_of(ref, state) * incoming
    incoming = incoming * decay_of(before_ref, state) + before_ref[0:state, :].astype(f32)
    incoming = incoming.astype(bf16)
    hot = one_hot(heads, widths)
    hot_mean = one_hot(heads, widths, mean=True)
    copies[0].wait()
    copies[1].wait()
    for i in range(length // size):
        here = slice(i * size, (i + 1) * size)
        grown = dot_first(jnp.exp(cum_ref[:, here]), hot, HIGH)
        parts = []
        offset = 0
        for kind, g_ref in enumerate((gs_ref, gl_ref)):
            there = slice(offset, offset + widths[kind])
            reads = maps_ref[here, (2 * kind + 1) * state : (2 * kind + 2) * state]
            scan = local_ref[here, there] + dot(reads, incoming[:, there]) * grown[:, there]
            parts.append(scan * silu(g_ref[here, :].astype(f32)))
            offset += widths[kind]
        squares = jnp.concatenate([part * part for part in parts], axis=1)
        scale = dot(lax.rsqrt(dot_last(squares, hot_mean, HIGH) + HEAD_EPS), hot, HIGH)
        offset = 0
        for part, h_ref in zip(parts, (hs_ref, hl_ref)):
            there = slice(offset, offset + part.shape[1])
            rows_ref[here, there] = (part * scale[:, there] * h_ref[...]).astype(bf16)
            offset += part.shape[1]
    place = place_ref[0]
    per = length // ways
    copies[2].wait()
    copies[3].wait()
    for slot in range(ways // 2):
        for bit, ref in ((1, send_ref), (0, keep_ref)):
            start = pl.multiple_of(jnp.bitwise_xor(place, 2 * slot + bit) * per, per)
            rows = rows_ref[pl.ds(start, per), :]
            part = dot(rows[:, : widths[0]], ws_ref[...]) + dot(rows[:, widths[0] :], wl_ref[...])
            ref[slot] = part.astype(bf16)


def norm_kernel(blocks, residual_ref, own_ref, other_ref, gain_ref, middle_ref, normed_ref):
    middle = residual_ref[...].astype(f32) + (own_ref[...].astype(f32) + other_ref[...].astype(f32))
    middle = middle.astype(bf16)
    middle_ref[...] = middle
    wide = middle.astype(f32)
    scale = lax.rsqrt(jnp.mean(wide * wide, axis=-1, keepdims=True) + ROW_EPS)
    normed = (wide * scale * gain_ref[...]).astype(bf16)
    width = normed.shape[1] // blocks
    for b in range(blocks):
        normed_ref[b] = normed[:, b * width : (b + 1) * width]


def last_kernel(group, count, pieces, place_ref, middle_ref, *refs):
    out_ref = refs[2 * group]
    deep = refs[0].shape[2]
    for k in range(group):
        own_ref, other_ref = refs[2 * k], refs[2 * k + 1]
        part = lax.rem(place_ref[0] - k + group, group)
        for b in range(count):
            first, second = b // pieces * group * pieces, b % pieces
            start = (first + part * pieces + second) * deep
            there = pl.ds(pl.multiple_of(start, deep), deep)
            added = own_ref[b].astype(f32) + other_ref[b].astype(f32)
            out_ref[:, there] = (middle_ref[:, there].astype(f32) + added).astype(bf16)


def hidden_kernel(blocks, pieces, index_ref, *refs):
    out_ref, gate_ref, up_ref, cat_ref, part_ref, sems = refs[-6:]
    chunks = refs[: len(refs) - 6 - 2 * blocks]
    weights = refs[len(chunks) : -6]
    rows, deep = chunks[0].shape[1:]
    depth = deep * pieces
    units = out_ref.shape[1]
    copies = []
    for kind, target in enumerate((gate_ref, up_ref)):
        for b in range(blocks):
            part = target.at[pl.ds(b * depth, depth), :]
            copies.append(pltpu.make_async_copy(weights[kind * blocks + b], part, sems.at[kind, b]))
    for copy in copies:
        copy.start()
    for kind, weight_ref in enumerate((gate_ref, up_ref)):
        for k in range(blocks * pieces):
            place = index_ref[kind * blocks * pieces + k]
            for j, chunk in enumerate(chunks):
                cat_ref[kind, j * rows : (j + 1) * rows, k * deep : (k + 1) * deep] = chunk[place]
        for copy in copies[kind * blocks : (kind + 1) * blocks]:
            copy.wait()
        tile = 256

        def some(here, kind=kind, weight_ref=weight_ref):
            value = dot(cat_ref[kind], weight_ref[:, here])
            if kind == 0:
                part_ref[:, here] = silu(value)
            else:
                out_ref[:, here] = (part_ref[:, here] * value).astype(bf16)

        def one(n, _, some=some):
            some(pl.ds(pl.multiple_of(n * tile, tile), tile))
            return 0

        lax.fori_loop(0, units // tile, one, 0)
        if units % tile:
            some(slice(units // tile * tile, units))


def down_kernel(blocks, pieces, start, parts, index_ref, *refs):
    hidden = refs[: len(parts)]
    weights = refs[len(parts) : len(parts) + blocks]
    outs = refs[len(parts) + blocks : 2 * len(parts) + blocks]
    down_ref, cat_ref, sems = refs[-3:]
    rows, deep = outs[0].shape[1:]
    copies = [pltpu.make_async_copy(weights[b], down_ref.at[b], sems.at[b]) for b in range(blocks)]
    for copy in copies:
        copy.start()
    for j, part in enumerate(parts):
        cat_ref[j * rows : (j + 1) * rows, :] = hidden[j][part * rows : (part + 1) * rows, :]
    for b in range(blocks):
        copies[b].wait()
        out = dot(cat_ref[...], down_ref[b]).astype(bf16)
        for k in range(pieces):
            place = index_ref[start + b * pieces + k]
            for j, ref in enumerate(outs):
                ref[place] = out[j * rows : (j + 1) * rows, k * deep : (k + 1) * deep]


def full(*arrays):
    return [pl.BlockSpec(a.shape, functools.partial(lambda n, i: (0,) * n, len(a.shape))) for a in arrays]


def params(mib):
    return pltpu.CompilerParams(vmem_limit_bytes=mib * 1024 * 1024)


def cost(flops, nbytes):
    return pl.CostEstimate(flops=int(flops), bytes_accessed=int(nbytes), transcendentals=0)


def on_device(sizes, residual, small_values, large_values, small_gates, large_gates, state_projections, small_steps, large_steps,
              small_offsets, large_offsets, small_rates, large_rates, small_taps, large_taps, state_taps, small_gains, large_gains,
              small_projection, large_projection, norm_gain, gate_matrix, up_matrix, down_matrix):
    n_sp, n_tp = sizes
    n_f = n_tp
    n_g = n_sp // n_f
    n_x = n_tp // 2
    sp = lax.axis_index("sp")
    tp = lax.axis_index("tp")
    g = lax.rem(sp, n_g)

    def send(x, to):
        pairs = []
        for s in range(n_sp):
            for t in range(n_tp):
                target = to(s // n_g, s % n_g, t)
                if target is not None:
                    pairs.append((s * n_tp + t, (target[0] * n_g + target[1]) * n_tp + target[2]))
        return lax.ppermute(x, AXES, pairs)

    def call(kernel, *args, **kw):
        return pl.pallas_call(kernel, **kw)(*args)

    def once(kernel, scalars, args, outs, scratch=(), mib=24, flops=4e9, far=()):
        return call(
            kernel,
            *scalars,
            *far,
            *args,
            grid=(1,),
            out_shape=tuple(outs),
            in_specs=[SMEM] * len(scalars) + [HBM] * len(far) + full(*args),
            out_specs=tuple(full(*outs)),
            scratch_shapes=list(scratch),
            compiler_params=params(mib),
            cost_estimate=cost(flops, 4e6),
        )

    length, width_small = small_values.shape
    width_large = large_values.shape[1]
    widths = (width_small, width_large)
    width = width_small + width_large
    heads = (small_rates.shape[0], large_rates.shape[0])
    planes, state = state_projections.shape[1:]
    rows, model = residual.shape

    last = length // HALO - 1
    edge = call(
        functools.partial(edge_kernel, state),
        small_values, large_values, state_projections,
        grid=(1,),
        out_shape=jax.ShapeDtypeStruct((HALO, width + planes * state), bf16),
        in_specs=[
            pl.BlockSpec((HALO, width_small), lambda i: (last, 0)),
            pl.BlockSpec((HALO, width_large), lambda i: (last, 0)),
            pl.BlockSpec((HALO, planes, state), lambda i: (last, 0, 0)),
        ],
        out_specs=pl.BlockSpec((HALO, width + planes * state), lambda i: (0, 0)),
    )
    halo = lax.ppermute(edge, "sp", [(i, i + 1) for i in range(n_sp - 1)])

    f = sp // n_g
    x = tp // 2
    c = lax.rem(tp, 2)
    pieces = 2 if n_x == 2 else 1
    blocks = n_sp
    deep = model // (blocks * pieces)

    def plane_of(x_, c_):
        return x_ + n_x * c_

    def slot_of(f_, plane, x_):
        if n_x != 2:
            return f_ % n_x, f_ // n_x
        k = f_ ^ plane
        return (x_ ^ 1 if k < 2 else x_), k % 2

    def moved(matrix, axis, split):
        if not split:

            def to(f_, g_, t_):
                plane = plane_of(t_ // 2, t_ % 2)
                x_, c_ = slot_of(f_, plane, t_ // 2)
                return plane, g_, 2 * x_ + c_

            return send(matrix, to)
        first = lax.slice_in_dim(matrix, 0, deep, axis=axis)
        second = lax.slice_in_dim(matrix, deep, 2 * deep, axis=axis)
        second = send(second, lambda f_, g_, t_: (f_, g_, t_ ^ 2))
        even = lax.rem(f, 2) == 0
        got = []
        for k, out in enumerate((jnp.where(even, first, second), jnp.where(even, second, first))):

            def to(f_, g_, t_, k=k):
                x_, c_ = t_ // 2, t_ % 2
                own = (f_ % 2 == 0) == (k == 0)
                return plane_of(x_ if own else 1 - x_, c_), g_, 2 * x_ + f_ // 2

            got.append(send(out, to))
        return jnp.concatenate(got, axis=axis)

    def gathered(matrix, axis, order, split):
        held = [(moved(matrix, axis, split), (0, 0, 0))]
        for kind in order:
            count = (n_x, n_g, 2)[kind]
            new = []
            for k in range(1, count):
                for block, way in held:
                    if kind == 0:
                        got = send(block, lambda f_, g_, t_: (f_, g_, 2 * ((t_ // 2 + k) % n_x) + t_ % 2))
                    elif kind == 1:
                        got = send(block, lambda f_, g_, t_: (f_, (g_ + k) % n_g, t_))
                    else:
                        got = send(block, lambda f_, g_, t_: (f_, g_, t_ ^ 1))
                    moved_by = list(way)
                    moved_by[kind] += k
                    new.append((got, tuple(moved_by)))
            held = held + new
        held.sort(key=lambda item: item[1][1])
        places = []
        for _, (dx, dg, dc) in held:
            x_ = lax.rem(x - dx + n_x, n_x)
            c_ = lax.rem(c - dc + 2, 2)
            g_ = lax.rem(g - dg + n_g, n_g)
            if split:
                own = lax.rem(f, 2) == x_
                for k in range(2):
                    f_ = 2 * c_ + jnp.where(own, k, 1 - k)
                    places.append((f_ * n_g + g_) * 2 + jnp.where(own, 0, 1))
                continue
            if n_x == 2:
                crossed = lax.rem(f, 2) != x_
                f_ = jnp.bitwise_xor(f, jnp.where(crossed, c_, 2 + c_))
            else:
                f_ = c_ * n_x + x_
            places += [(f_ * n_g + g_) * pieces + k for k in range(pieces)]
        return [block for block, _ in held], places

    two = n_x == 2
    gates, gate_places = gathered(gate_matrix, 0, (0, 1, 2), False)
    ups, up_places = gathered(up_matrix, 0, (1, 0, 2), two)
    downs, down_places = gathered(down_matrix, 1, (0, 1, 2), two)
    index = jnp.stack(gate_places + up_places + down_places).astype(jnp.int32)

    message = jax.ShapeDtypeStruct((state + EXTRA, width), bf16)
    per_head = (padded(sum(heads)), length)
    driven, maps, cum, own = once(
        functools.partial(start_kernel, widths, heads, state),
        (small_rates, large_rates),
        (halo, small_values, large_values, state_projections, small_steps.T, large_steps.T, small_offsets.T, large_offsets.T,
         small_taps, large_taps, state_taps),
        (
            jax.ShapeDtypeStruct((length, width), bf16),
            jax.ShapeDtypeStruct((length, planes * state), bf16),
            jax.ShapeDtypeStruct(per_head, f32),
            message,
        ),
        (pltpu.VMEM((HALO + length, max(widths + (state,))), f32), pltpu.VMEM(per_head, f32)),
    )
    others = [send(own, lambda f_, g_, t_: (f_, (g_ + k) % n_g, t_)) for k in range(1, n_g)]
    (local,) = once(
        functools.partial(local_kernel, widths, heads, state),
        (),
        (driven, maps, cum),
        (jax.ShapeDtypeStruct((length, width), f32),),
    )
    joined, before = once(
        functools.partial(group_kernel, n_g, state), (g[None].astype(jnp.int32),), (own, *others), (message, message)
    )
    arrived = [send(joined, lambda f_, g_, t_: (f_ + k, g_, t_) if f_ + k < n_f else None) for k in range(1, n_f)]

    half = n_tp // 2
    part = jax.ShapeDtypeStruct((half, rows, model), bf16)
    keep, give = once(
        functools.partial(finish_kernel, widths, heads, state, n_tp, len(arrived)),
        (tp[None].astype(jnp.int32),),
        (local, maps, cum, small_gains[None, :], large_gains[None, :], before, *arrived),
        (part, part),
        (
            pltpu.VMEM((length, width), bf16),
            pltpu.VMEM(small_gates.shape, bf16),
            pltpu.VMEM(large_gates.shape, bf16),
            pltpu.VMEM(small_projection.shape, bf16),
            pltpu.VMEM(large_projection.shape, bf16),
            pltpu.SemaphoreType.DMA((4,)),
        ),
        mib=32,
        far=(small_gates, large_gates, small_projection, large_projection),
    )

    got = send(give, lambda f_, g_, t_: (f_, g_, t_ ^ 1))
    kept = [keep[i] for i in range(half)]
    arriving = [got[i] for i in range(half)]
    bit = 2
    while len(kept) > 1:
        sent = []
        stay = []
        for i in range(0, len(kept), 2):
            stay.append((kept[i].astype(f32) + arriving[i].astype(f32)).astype(bf16))
            sent.append((kept[i + 1].astype(f32) + arriving[i + 1].astype(f32)).astype(bf16))
        arriving = [send(x, lambda f_, g_, t_, b=bit: (f_, g_, t_ ^ b)) for x in sent]
        kept = stay
        bit *= 2
    chunk_shape = jax.ShapeDtypeStruct((blocks * pieces, rows, deep), bf16)
    middle, normed = once(
        functools.partial(norm_kernel, blocks * pieces),
        (),
        (residual, kept[0], arriving[0], norm_gain[None, :]),
        (jax.ShapeDtypeStruct((rows, model), bf16), chunk_shape),
    )

    units = gate_matrix.shape[1]
    each = blocks // n_g

    def ring(x):
        return send(x, lambda f_, g_, t_: ((f_ + 1) % n_f, g_, t_))

    chunks = [normed]
    for _ in range(1, n_f):
        chunks.append(ring(chunks[-1]))

    def hidden_of(*which):
        count = len(which) * rows
        return call(
            functools.partial(hidden_kernel, blocks, pieces),
            index, *(chunks[s] for s in which), *gates, *ups,
            out_shape=jax.ShapeDtypeStruct((count, units), bf16),
            in_specs=[SMEM] + [VMEM] * len(which) + [HBM] * (2 * blocks),
            out_specs=VMEM,
            scratch_shapes=[
                pltpu.VMEM((model, units), bf16),
                pltpu.VMEM((model, units), bf16),
                pltpu.VMEM((2, count, model), bf16),
                pltpu.VMEM((count, units), f32),
                pltpu.SemaphoreType.DMA((2, blocks)),
            ],
            compiler_params=params(28),
            cost_estimate=cost(4 * count * model * units, 12e6),
        )

    local_places = jnp.stack([place // (n_g * pieces) * pieces + lax.rem(place, pieces) for place in down_places]).astype(jnp.int32)

    def down_of(k, *hidden):
        part = jax.ShapeDtypeStruct((each * pieces, rows, deep), bf16)
        return call(
            functools.partial(down_kernel, each, pieces, k * each * pieces, tuple(p for _, p in hidden)),
            local_places, *(h for h, _ in hidden), *downs[k * each : (k + 1) * each],
            out_shape=(part,) * len(hidden),
            in_specs=[SMEM] + [VMEM] * len(hidden) + [HBM] * each,
            out_specs=(VMEM,) * len(hidden),
            scratch_shapes=[
                pltpu.VMEM((each, units, deep * pieces), bf16),
                pltpu.VMEM((len(hidden) * rows, units), bf16),
                pltpu.SemaphoreType.DMA((each,)),
            ],
            compiler_params=params(20),
            cost_estimate=cost(2 * len(hidden) * rows * model * units // n_g, 6e6 // n_g),
        )

    hidden = [hidden_of(1, 0)] + [hidden_of(s) for s in range(2, n_f)]
    sums = []
    for k in range(n_g):
        (total,) = down_of(k, (hidden[0], 0))
        for s in range(2, n_f):
            more = [(hidden[s - 1], 0)] + ([(hidden[0], 1)] if s == n_f - 1 else [])
            added, *own = down_of(k, *more)
            total = (ring(total).astype(f32) + added.astype(f32)).astype(bf16)
        sums += [own[0], ring(total)]
    (out,) = once(
        functools.partial(last_kernel, n_g, each * pieces, pieces),
        (g[None].astype(jnp.int32),),
        (middle, *sums),
        (jax.ShapeDtypeStruct((rows, model), bf16),),
    )
    return out


def solution(mesh):
    sizes = (mesh.shape["sp"], mesh.shape["tp"])
    in_specs = (
        P(AXES, None),
        P("sp", "tp"), P("sp", "tp"), P("sp", "tp"), P("sp", "tp"),
        P("sp", None, None),
        P("sp", "tp"), P("sp", "tp"), P("sp", "tp"), P("sp", "tp"),
        P("tp"), P("tp"),
        P(None, "tp"), P(None, "tp"),
        P(),
        P("tp"), P("tp"),
        P("tp", None), P("tp", None),
        P(),
        P("sp", "tp"), P("sp", "tp"), P("tp", "sp"),
    )

    def layer(*args):
        return on_device(sizes, *args)

    return jax.shard_map(layer, mesh=mesh, in_specs=in_specs, out_specs=P(AXES, None), check_vma=False)
```

```python
import functools

import jax
import jax.numpy as jnp
from jax import lax
from jax.experimental import pallas as pl
from jax.experimental.pallas import tpu as pltpu
from jax.sharding import PartitionSpec as P


HIGH = lax.Precision.HIGHEST
HEAD_EPS = 1e-05
ROW_EPS = 1e-06
HALO = 8
EXTRA = 16
AXES = ("sp", "tp")


f32 = jnp.float32
bf16 = jnp.bfloat16
VMEM = pl.BlockSpec(memory_space=pltpu.VMEM)
SMEM = pl.BlockSpec(memory_space=pltpu.SMEM)
HBM = pl.BlockSpec(memory_space=pltpu.HBM)
ANY = pl.BlockSpec(memory_space=pl.ANY)


def block_of(length):
    for size in (128, 64, 32, 16, 8):
        if length % size == 0:
            return size
    return length


def dot(a, b, precision=None):
    return jnp.dot(a, b, preferred_element_type=f32, precision=precision)


def dot_first(a, b, precision=None):
    return lax.dot_general(a, b, (((0,), (0,)), ((), ())), preferred_element_type=f32, precision=precision)


def dot_last(a, b, precision=None):
    return lax.dot_general(a, b, (((1,), (1,)), ((), ())), preferred_element_type=f32, precision=precision)


def one_hot(heads, widths, mean=False):
    count = padded(sum(heads))
    total = sum(widths)
    head = lax.broadcasted_iota(jnp.int32, (count, total), 0)
    channel = lax.broadcasted_iota(jnp.int32, (count, total), 1)
    hot = jnp.zeros((count, total), f32)
    first, start = 0, 0
    for number, width in zip(heads, widths):
        size = width // number
        low = start + (head - first) * size
        inside = (head >= first) & (head < first + number) & (channel >= low) & (channel < low + size)
        hot = jnp.where(inside, 1.0 / size if mean else 1.0, hot)
        first += number
        start += width
    return hot


def padded(count):
    return -(-count // 8) * 8


def silu(x):
    return x * (1.0 / (1.0 + jnp.exp(-x)))


def conv(pad_ref, halo, series, taps):
    length, width = series.shape
    pad_ref[0:HALO, 0:width] = halo.astype(f32)
    pad_ref[HALO : HALO + length, 0:width] = series.astype(f32)
    total = jnp.zeros((length, width), f32)
    for k, tap in enumerate(taps):
        first = HALO - (len(taps) - 1) + k
        total = total + tap.astype(f32) * pad_ref[first : first + length, 0:width]
    return silu(total)


def softplus(x):
    return jnp.maximum(x, 0.0) + jnp.log1p(jnp.exp(-jnp.abs(x)))


def edge_kernel(state, vs_ref, vl_ref, proj_ref, out_ref):
    first = vs_ref.shape[1]
    second = first + vl_ref.shape[1]
    out_ref[:, :first] = vs_ref[...]
    out_ref[:, first:second] = vl_ref[...]
    for plane in range(proj_ref.shape[1]):
        lo = second + plane * state
        out_ref[:, lo : lo + state] = proj_ref[:, plane, :]


def start_kernel(widths, heads, state, rs_ref, rl_ref, halo_ref, vs_ref, vl_ref, proj_ref, ss_ref, sl_ref, os_ref, ol_ref,
                 ts_ref, tl_ref, tm_ref, driven_ref, maps_ref, cum_ref, msg_ref, pad_ref, step_ref):
    length = vs_ref.shape[0]
    size = block_of(length)
    step_ref[...] = jnp.zeros_like(step_ref)
    cum_ref[...] = jnp.zeros_like(cum_ref)
    first = 0
    for number, s_ref, o_ref, r_ref in ((heads[0], ss_ref, os_ref, rs_ref), (heads[1], sl_ref, ol_ref, rl_ref)):
        step = softplus(s_ref[...].astype(f32))
        step_ref[first : first + number, :] = step
        for h in range(number):
            rate = jnp.exp(jnp.full((1, length), r_ref[h], f32))
            cum_ref[first + h : first + h + 1, :] = o_ref[h : h + 1, :] - rate * step[h : h + 1, :]
        first += number
    row = lax.broadcasted_iota(jnp.int32, (size, size), 0)
    col = lax.broadcasted_iota(jnp.int32, (size, size), 1)
    tri = jnp.where(row <= col, 1.0, 0.0).astype(f32)
    base = jnp.zeros((cum_ref.shape[0], 1), f32)
    for i in range(length // size):
        within = dot(cum_ref[:, i * size : (i + 1) * size], tri, HIGH) + base
        cum_ref[:, i * size : (i + 1) * size] = within
        base = within[:, size - 1 : size]
    hot = one_hot(heads, widths)
    count = tm_ref.shape[0]
    for plane in range(4):
        lo = plane * state
        at = sum(widths) + lo
        taps = [tm_ref[k, plane : plane + 1, :] for k in range(count)]
        done = conv(pad_ref, halo_ref[:, at : at + state], proj_ref[:, plane, :], taps)
        maps_ref[:, lo : lo + state] = done.astype(bf16)
    steps = dot_first(step_ref[...], hot, HIGH)
    tails = dot_first(jnp.exp(base - cum_ref[...]), hot, HIGH)
    offset = 0
    for kind, (width, v_ref, t_ref) in enumerate(((widths[0], vs_ref, ts_ref), (widths[1], vl_ref, tl_ref))):
        there = slice(offset, offset + width)
        taps = [t_ref[k : k + 1, :] for k in range(count)]
        driven = conv(pad_ref, halo_ref[:, there], v_ref[...], taps) * steps[:, there]
        driven_ref[:, there] = driven.astype(bf16)
        keys = maps_ref[:, 2 * kind * state : (2 * kind + 1) * state]
        msg_ref[0:state, there] = dot_first(keys, (driven * tails[:, there]).astype(bf16)).astype(bf16)
        offset += width
    write_decay(msg_ref, state, dot_first(jnp.exp(base), hot, HIGH))


def write_decay(ref, state, decay):
    high = decay.astype(bf16).astype(f32)
    index = lax.broadcasted_iota(jnp.int32, (EXTRA, decay.shape[1]), 0)
    rows = jnp.where(index == 0, high, jnp.where(index == 1, decay - high, 0.0))
    ref[state : state + EXTRA, :] = rows.astype(bf16)


def decay_of(ref, state):
    return ref[state : state + 1, :].astype(f32) + ref[state + 1 : state + 2, :].astype(f32)


def local_kernel(widths, heads, state, driven_ref, maps_ref, cum_ref, out_ref):
    length = driven_ref.shape[0]
    size = block_of(length)
    row = lax.broadcasted_iota(jnp.int32, (size, size), 0)
    col = lax.broadcasted_iota(jnp.int32, (size, size), 1)
    mask = row >= col
    hot = one_hot(heads, widths)
    base = jnp.zeros((cum_ref.shape[0], 1), f32)
    carry = [jnp.zeros((state, width), f32) for width in widths]
    for i in range(length // size):
        here = slice(i * size, (i + 1) * size)
        within = cum_ref[:, here] - base
        down = within.T
        last = within[:, size - 1 : size]
        grown = dot_first(jnp.exp(within), hot, HIGH)
        tails = dot_first(jnp.exp(last - within), hot, HIGH)
        whole = grown[size - 1 : size, :]
        base = base + last
        offset, first = 0, 0
        for kind in range(2):
            width, number = widths[kind], heads[kind]
            each = width // number
            there = slice(offset, offset + width)
            keys = maps_ref[here, 2 * kind * state : (2 * kind + 1) * state]
            reads = maps_ref[here, (2 * kind + 1) * state : (2 * kind + 2) * state]
            driven = driven_ref[here, there]
            scores = dot_last(reads, keys)
            parts = []
            for h in range(number):
                gap = down[:, first + h : first + h + 1] - within[first + h : first + h + 1, :]
                weights = jnp.where(mask, jnp.exp(jnp.where(mask, gap, 0.0)), 0.0)
                parts.append(dot((scores * weights).astype(bf16), driven[:, h * each : (h + 1) * each]))
            inner = jnp.concatenate(parts, axis=1) if number > 1 else parts[0]
            if i > 0:
                inner = inner + dot(reads, carry[kind].astype(bf16)) * grown[:, there]
            out_ref[here, there] = inner
            if i + 1 < length // size:
                fresh = (driven.astype(f32) * tails[:, there]).astype(bf16)
                carry[kind] = carry[kind] * whole[:, there] + dot_first(keys, fresh)
            offset += width
            first += number


def group_kernel(group, state, place_ref, *refs):
    out_ref, before_ref = refs[group], refs[group + 1]
    place = place_ref[0]
    places = [lax.rem(place - k + group, group) for k in range(group)]
    decays = [decay_of(ref, state) for ref in refs[:group]]
    ones = jnp.ones_like(decays[0])
    total = jnp.zeros((state, ones.shape[1]), f32)
    before = jnp.zeros_like(total)
    total_decay = ones
    before_decay = ones
    for k in range(group):
        rest = ones
        rest_before = ones
        for m in range(group):
            if m != k:
                rest = jnp.where(places[m] > places[k], rest * decays[m], rest)
                rest_before = jnp.where((places[m] > places[k]) & (places[m] < place), rest_before * decays[m], rest_before)
        values = refs[k][0:state, :].astype(f32)
        total = total + values * rest
        total_decay = total_decay * decays[k]
        if k > 0:
            is_before = places[k] < place
            before = before + jnp.where(is_before, values * rest_before, 0.0)
            before_decay = jnp.where(is_before, before_decay * decays[k], before_decay)
    for ref, values, decay in ((out_ref, total, total_decay), (before_ref, before, before_decay)):
        ref[0:state, :] = values.astype(bf16)
        write_decay(ref, state, decay)


def finish_kernel(widths, heads, state, ways, hops, place_ref, gs_far, gl_far, ws_far, wl_far, local_ref, maps_ref, cum_ref,
                  hs_ref, hl_ref, before_ref, *refs):
    arrived = refs[:hops]
    keep_ref, send_ref, rows_ref, gs_ref, gl_ref, ws_ref, wl_ref, sems = refs[hops:]
    pairs = ((gs_far, gs_ref), (gl_far, gl_ref), (ws_far, ws_ref), (wl_far, wl_ref))
    copies = [pltpu.make_async_copy(far, near, sems.at[k]) for k, (far, near) in enumerate(pairs)]
    for copy in copies:
        copy.start()
    length = local_ref.shape[0]
    size = block_of(length)
    incoming = jnp.zeros((state, local_ref.shape[1]), f32)
    for ref in reversed(arrived):
        incoming = ref[0:state, :].astype(f32) + decay_of(ref, state) * incoming
    incoming = incoming * decay_of(before_ref, state) + before_ref[0:state, :].astype(f32)
    incoming = incoming.astype(bf16)
    hot = one_hot(heads, widths)
    hot_mean = one_hot(heads, widths, mean=True)
    copies[0].wait()
    copies[1].wait()
    for i in range(length // size):
        here = slice(i * size, (i + 1) * size)
        grown = dot_first(jnp.exp(cum_ref[:, here]), hot, HIGH)
        parts = []
        offset = 0
        for kind, g_ref in enumerate((gs_ref, gl_ref)):
            there = slice(offset, offset + widths[kind])
            reads = maps_ref[here, (2 * kind + 1) * state : (2 * kind + 2) * state]
            scan = local_ref[here, there] + dot(reads, incoming[:, there]) * grown[:, there]
            parts.append(scan * silu(g_ref[here, :].astype(f32)))
            offset += widths[kind]
        squares = jnp.concatenate([part * part for part in parts], axis=1)
        scale = dot(lax.rsqrt(dot_last(squares, hot_mean, HIGH) + HEAD_EPS), hot, HIGH)
        offset = 0
        for part, h_ref in zip(parts, (hs_ref, hl_ref)):
            there = slice(offset, offset + part.shape[1])
            rows_ref[here, there] = (part * scale[:, there] * h_ref[...]).astype(bf16)
            offset += part.shape[1]
    place = place_ref[0]
    per = length // ways
    copies[2].wait()
    copies[3].wait()
    for slot in range(ways // 2):
        for bit, ref in ((1, send_ref), (0, keep_ref)):
            start = pl.multiple_of(jnp.bitwise_xor(place, 2 * slot + bit) * per, per)
            rows = rows_ref[pl.ds(start, per), :]
            part = dot(rows[:, : widths[0]], ws_ref[...]) + dot(rows[:, widths[0] :], wl_ref[...])
            ref[slot] = part.astype(bf16)


def norm_kernel(blocks, residual_ref, own_ref, other_ref, gain_ref, middle_ref, normed_ref):
    middle = residual_ref[...].astype(f32) + (own_ref[...].astype(f32) + other_ref[...].astype(f32))
    middle = middle.astype(bf16)
    middle_ref[...] = middle
    wide = middle.astype(f32)
    scale = lax.rsqrt(jnp.mean(wide * wide, axis=-1, keepdims=True) + ROW_EPS)
    normed = (wide * scale * gain_ref[...]).astype(bf16)
    width = normed.shape[1] // blocks
    for b in range(blocks):
        normed_ref[b] = normed[:, b * width : (b + 1) * width]


def join_kernel(axis, first_ref, second_ref, out_ref, sems):
    copies = []
    for k, ref in enumerate((first_ref, second_ref)):
        there = pl.ds(k * ref.shape[axis], ref.shape[axis])
        target = out_ref.at[there, :] if axis == 0 else out_ref.at[:, there]
        copies.append(pltpu.make_async_copy(ref, target, sems.at[k]))
    for copy in copies:
        copy.start()
    for copy in copies:
        copy.wait()


def last_kernel(group, count, pieces, place_ref, middle_ref, *refs):
    out_ref = refs[2 * group]
    deep = refs[0].shape[2]
    for k in range(group):
        own_ref, other_ref = refs[2 * k], refs[2 * k + 1]
        part = lax.rem(place_ref[0] - k + group, group)
        for b in range(count):
            first, second = b // pieces * group * pieces, b % pieces
            start = (first + part * pieces + second) * deep
            there = pl.ds(pl.multiple_of(start, deep), deep)
            added = own_ref[b].astype(f32) + other_ref[b].astype(f32)
            out_ref[:, there] = (middle_ref[:, there].astype(f32) + added).astype(bf16)


def hidden_kernel(blocks, pieces, kinds, index_ref, *refs):
    out_ref, weight_ref, cat_ref, part_ref, chunks_ref, sems = refs[-6:]
    inputs = refs[:-6]
    weights = inputs[len(inputs) - len(kinds) * blocks :]
    far = inputs[: len(inputs) - len(kinds) * blocks]
    rows, deep = chunks_ref.shape[2:]
    depth = deep * pieces
    units = out_ref.shape[1]
    tile = 256
    cut = units // (2 * tile) * tile
    spans = ((0, cut), (cut, units)) if cut else ((0, units),)
    arrivals = []
    if kinds == (1,):
        arrivals.append(pltpu.make_async_copy(far[-1], part_ref, sems.at[2, 0, blocks - 1]))
        far = far[:-1]
    arrivals += [pltpu.make_async_copy(ref, chunks_ref.at[j], sems.at[2, 0, j]) for j, ref in enumerate(far)]
    copies = []
    for n in range(len(kinds)):
        for p, (low, high) in enumerate(spans):
            for b in range(blocks):
                source = weights[n * blocks + b].at[:, low:high]
                target = weight_ref.at[n, pl.ds(b * depth, depth), low:high]
                copies.append(pltpu.make_async_copy(source, target, sems.at[n, p, b]))
    for copy in arrivals + copies:
        copy.start()
    for copy in arrivals:
        copy.wait()
    for n, kind in enumerate(kinds):
        for k in range(blocks * pieces):
            place = index_ref[kind * blocks * pieces + k]
            for j in range(len(far)):
                cat_ref[n, j * rows : (j + 1) * rows, k * deep : (k + 1) * deep] = chunks_ref[j, place]

        def some(here, n=n, kind=kind):
            value = dot(cat_ref[n], weight_ref[n, :, here])
            if kind == 1:
                out_ref[:, here] = (part_ref[:, here] * value).astype(bf16)
            elif len(kinds) == 2:
                part_ref[:, here] = silu(value)
            else:
                out_ref[:, here] = silu(value)

        def one(i, _, some=some):
            some(pl.ds(pl.multiple_of(i * tile, tile), tile))
            return 0

        for p, (low, high) in enumerate(spans):
            for copy in copies[(n * len(spans) + p) * blocks : (n * len(spans) + p + 1) * blocks]:
                copy.wait()
            lax.fori_loop(low // tile, high // tile, one, 0)
            if high % tile:
                some(slice(high // tile * tile, high))


def down_kernel(blocks, pieces, start, parts, index_ref, *refs):
    hidden = refs[: len(parts)]
    weights = refs[len(parts) : len(parts) + blocks]
    outs = refs[len(parts) + blocks : 2 * len(parts) + blocks]
    down_ref, cat_ref, sems = refs[-3:]
    rows, deep = outs[0].shape[1:]
    copies = [pltpu.make_async_copy(weights[b], down_ref.at[b], sems.at[b]) for b in range(blocks)]
    for copy in copies:
        copy.start()
    for j, part in enumerate(parts):
        cat_ref[j * rows : (j + 1) * rows, :] = hidden[j][part * rows : (part + 1) * rows, :]
    for b in range(blocks):
        copies[b].wait()
        out = dot(cat_ref[...], down_ref[b]).astype(bf16)
        for k in range(pieces):
            place = index_ref[start + b * pieces + k]
            for j, ref in enumerate(outs):
                ref[place] = out[j * rows : (j + 1) * rows, k * deep : (k + 1) * deep]


def full(*arrays):
    return [pl.BlockSpec(a.shape, functools.partial(lambda n, i: (0,) * n, len(a.shape))) for a in arrays]


def params(mib):
    return pltpu.CompilerParams(vmem_limit_bytes=mib * 1024 * 1024)


def cost(flops, nbytes):
    return pl.CostEstimate(flops=int(flops), bytes_accessed=int(nbytes), transcendentals=0)


def on_device(sizes, residual, small_values, large_values, small_gates, large_gates, state_projections, small_steps, large_steps,
              small_offsets, large_offsets, small_rates, large_rates, small_taps, large_taps, state_taps, small_gains, large_gains,
              small_projection, large_projection, norm_gain, gate_matrix, up_matrix, down_matrix):
    n_sp, n_tp = sizes
    n_f = n_tp
    n_g = n_sp // n_f
    n_x = n_tp // 2
    sp = lax.axis_index("sp")
    tp = lax.axis_index("tp")
    g = lax.rem(sp, n_g)

    def send(x, to):
        pairs = []
        for s in range(n_sp):
            for t in range(n_tp):
                target = to(s // n_g, s % n_g, t)
                if target is not None:
                    pairs.append((s * n_tp + t, (target[0] * n_g + target[1]) * n_tp + target[2]))
        return lax.ppermute(x, AXES, pairs)

    def call(kernel, *args, **kw):
        return pl.pallas_call(kernel, **kw)(*args)

    def once(kernel, scalars, args, outs, scratch=(), mib=24, flops=4e9, far=()):
        return call(
            kernel,
            *scalars,
            *far,
            *args,
            grid=(1,),
            out_shape=tuple(outs),
            in_specs=[SMEM] * len(scalars) + [HBM] * len(far) + full(*args),
            out_specs=tuple(full(*outs)),
            scratch_shapes=list(scratch),
            compiler_params=params(mib),
            cost_estimate=cost(flops, 4e6),
        )

    length, width_small = small_values.shape
    width_large = large_values.shape[1]
    widths = (width_small, width_large)
    width = width_small + width_large
    heads = (small_rates.shape[0], large_rates.shape[0])
    planes, state = state_projections.shape[1:]
    rows, model = residual.shape

    last = length // HALO - 1
    edge = call(
        functools.partial(edge_kernel, state),
        small_values, large_values, state_projections,
        grid=(1,),
        out_shape=jax.ShapeDtypeStruct((HALO, width + planes * state), bf16),
        in_specs=[
            pl.BlockSpec((HALO, width_small), lambda i: (last, 0)),
            pl.BlockSpec((HALO, width_large), lambda i: (last, 0)),
            pl.BlockSpec((HALO, planes, state), lambda i: (last, 0, 0)),
        ],
        out_specs=pl.BlockSpec((HALO, width + planes * state), lambda i: (0, 0)),
    )
    halo = lax.ppermute(edge, "sp", [(i, i + 1) for i in range(n_sp - 1)])

    f = sp // n_g
    x = tp // 2
    c = lax.rem(tp, 2)
    pieces = 2 if n_x == 2 else 1
    blocks = n_sp
    deep = model // (blocks * pieces)

    def plane_of(x_, c_):
        return x_ + n_x * c_

    def slot_of(f_, plane, x_):
        if n_x != 2:
            return f_ % n_x, f_ // n_x
        k = f_ ^ plane
        return (x_ ^ 1 if k < 2 else x_), k % 2

    def moved(matrix, axis, split):
        if not split:

            def to(f_, g_, t_):
                plane = plane_of(t_ // 2, t_ % 2)
                x_, c_ = slot_of(f_, plane, t_ // 2)
                return plane, g_, 2 * x_ + c_

            return send(matrix, to)
        first = lax.slice_in_dim(matrix, 0, deep, axis=axis)
        second = lax.slice_in_dim(matrix, deep, 2 * deep, axis=axis)
        second = send(second, lambda f_, g_, t_: (f_, g_, t_ ^ 2))
        even = lax.rem(f, 2) == 0
        got = []
        for k, out in enumerate((jnp.where(even, first, second), jnp.where(even, second, first))):

            def to(f_, g_, t_, k=k):
                x_, c_ = t_ // 2, t_ % 2
                own = (f_ % 2 == 0) == (k == 0)
                return plane_of(x_ if own else 1 - x_, c_), g_, 2 * x_ + f_ // 2

            got.append(send(out, to))
        return joined_of(axis, *got)

    def joined_of(axis, *parts):
        shape = tuple(2 * deep if i == axis else n for i, n in enumerate(parts[0].shape))
        return call(
            functools.partial(join_kernel, axis),
            *parts,
            out_shape=jax.ShapeDtypeStruct(shape, bf16),
            in_specs=[HBM] * 2,
            out_specs=HBM,
            scratch_shapes=[pltpu.SemaphoreType.DMA((2,))],
            compiler_params=params(4),
            cost_estimate=cost(1e6, 3e6),
        )

    def gathered(matrix, axis, order, split, both=False):
        held = [(moved(matrix, axis, split), (0, 0, 0))]
        if both:
            def over_x(block):
                return send(block, lambda f_, g_, t_: (f_, g_, t_ ^ 2))

            def over_g(block):
                return send(block, lambda f_, g_, t_: (f_, 1 - g_, t_))

            own = held[0][0]
            one, other = over_x(own), over_g(own)
            first = over_g(lax.slice_in_dim(one, 0, deep, axis=axis))
            second = over_x(lax.slice_in_dim(other, deep, 2 * deep, axis=axis))
            held += [(one, (1, 0, 0)), (other, (0, 1, 0)), (joined_of(axis, first, second), (1, 1, 0))]
            order = (2,)
        for kind in order:
            count = (n_x, n_g, 2)[kind]
            new = []
            for k in range(1, count):
                for block, way in held:
                    if kind == 0:
                        got = send(block, lambda f_, g_, t_: (f_, g_, 2 * ((t_ // 2 + k) % n_x) + t_ % 2))
                    elif kind == 1:
                        got = send(block, lambda f_, g_, t_: (f_, (g_ + k) % n_g, t_))
                    else:
                        got = send(block, lambda f_, g_, t_: (f_, g_, t_ ^ 1))
                    moved_by = list(way)
                    moved_by[kind] += k
                    new.append((got, tuple(moved_by)))
            held = held + new
        held.sort(key=lambda item: item[1][1])
        places = []
        for _, (dx, dg, dc) in held:
            x_ = lax.rem(x - dx + n_x, n_x)
            c_ = lax.rem(c - dc + 2, 2)
            g_ = lax.rem(g - dg + n_g, n_g)
            if split:
                own = lax.rem(f, 2) == x_
                for k in range(2):
                    f_ = 2 * c_ + jnp.where(own, k, 1 - k)
                    places.append((f_ * n_g + g_) * 2 + jnp.where(own, 0, 1))
                continue
            if n_x == 2:
                crossed = lax.rem(f, 2) != x_
                f_ = jnp.bitwise_xor(f, jnp.where(crossed, c_, 2 + c_))
            else:
                f_ = c_ * n_x + x_
            places += [(f_ * n_g + g_) * pieces + k for k in range(pieces)]
        return [block for block, _ in held], places

    two = n_x == 2
    gates, gate_places = gathered(gate_matrix, 0, (0, 1, 2), False)
    ups, up_places = gathered(up_matrix, 0, (0, 1, 2), two, two and n_g == 2)
    downs, down_places = gathered(down_matrix, 1, (0, 1, 2), two)
    index = jnp.stack(gate_places + up_places + down_places).astype(jnp.int32)

    message = jax.ShapeDtypeStruct((state + EXTRA, width), bf16)
    per_head = (padded(sum(heads)), length)
    driven, maps, cum, own = once(
        functools.partial(start_kernel, widths, heads, state),
        (small_rates, large_rates),
        (halo, small_values, large_values, state_projections, small_steps.T, large_steps.T, small_offsets.T, large_offsets.T,
         small_taps, large_taps, state_taps),
        (
            jax.ShapeDtypeStruct((length, width), bf16),
            jax.ShapeDtypeStruct((length, planes * state), bf16),
            jax.ShapeDtypeStruct(per_head, f32),
            message,
        ),
        (pltpu.VMEM((HALO + length, max(widths + (state,))), f32), pltpu.VMEM(per_head, f32)),
    )
    others = [send(own, lambda f_, g_, t_: (f_, (g_ + k) % n_g, t_)) for k in range(1, n_g)]
    (local,) = once(
        functools.partial(local_kernel, widths, heads, state),
        (),
        (driven, maps, cum),
        (jax.ShapeDtypeStruct((length, width), f32),),
    )
    joined, before = once(
        functools.partial(group_kernel, n_g, state), (g[None].astype(jnp.int32),), (own, *others), (message, message)
    )
    arrived = [send(joined, lambda f_, g_, t_: (f_ + k, g_, t_) if f_ + k < n_f else None) for k in range(1, n_f)]

    half = n_tp // 2
    part = jax.ShapeDtypeStruct((half, rows, model), bf16)
    keep, give = once(
        functools.partial(finish_kernel, widths, heads, state, n_tp, len(arrived)),
        (tp[None].astype(jnp.int32),),
        (local, maps, cum, small_gains[None, :], large_gains[None, :], before, *arrived),
        (part, part),
        (
            pltpu.VMEM((length, width), bf16),
            pltpu.VMEM(small_gates.shape, bf16),
            pltpu.VMEM(large_gates.shape, bf16),
            pltpu.VMEM(small_projection.shape, bf16),
            pltpu.VMEM(large_projection.shape, bf16),
            pltpu.SemaphoreType.DMA((4,)),
        ),
        mib=32,
        far=(small_gates, large_gates, small_projection, large_projection),
    )

    got = send(give, lambda f_, g_, t_: (f_, g_, t_ ^ 1))
    kept = [keep[i] for i in range(half)]
    arriving = [got[i] for i in range(half)]
    bit = 2
    while len(kept) > 1:
        sent = []
        stay = []
        for i in range(0, len(kept), 2):
            stay.append((kept[i].astype(f32) + arriving[i].astype(f32)).astype(bf16))
            sent.append((kept[i + 1].astype(f32) + arriving[i + 1].astype(f32)).astype(bf16))
        arriving = [send(x, lambda f_, g_, t_, b=bit: (f_, g_, t_ ^ b)) for x in sent]
        kept = stay
        bit *= 2
    chunk_shape = jax.ShapeDtypeStruct((blocks * pieces, rows, deep), bf16)
    middle, normed = once(
        functools.partial(norm_kernel, blocks * pieces),
        (),
        (residual, kept[0], arriving[0], norm_gain[None, :]),
        (jax.ShapeDtypeStruct((rows, model), bf16), chunk_shape),
    )

    units = gate_matrix.shape[1]
    each = blocks // n_g

    def ring(x):
        return send(x, lambda f_, g_, t_: ((f_ + 1) % n_f, g_, t_))

    chunks = [normed]
    for _ in range(1, n_f):
        chunks.append(ring(chunks[-1]))

    def hidden_of(which, kinds=(0, 1), first=()):
        count = len(which) * rows
        weights = [block for kind in kinds for block in (gates, ups)[kind]]
        return call(
            functools.partial(hidden_kernel, blocks, pieces, kinds),
            index, *(chunks[s] for s in which), *first, *weights,
            out_shape=jax.ShapeDtypeStruct((count, units), f32 if kinds == (0,) else bf16),
            in_specs=[SMEM] + [ANY] * (len(which) + len(first)) + [HBM] * len(weights),
            out_specs=VMEM,
            scratch_shapes=[
                pltpu.VMEM((len(kinds), model, units), bf16),
                pltpu.VMEM((len(kinds), count, model), bf16),
                pltpu.VMEM((count, units), f32),
                pltpu.VMEM((len(which), blocks * pieces, rows, deep), bf16),
                pltpu.SemaphoreType.DMA((3, 2, blocks)),
            ],
            compiler_params=params(28 if len(kinds) == 2 else 56),
            cost_estimate=cost(2 * len(kinds) * count * model * units, 6e6 * len(kinds)),
        )

    local_places = jnp.stack([place // (n_g * pieces) * pieces + lax.rem(place, pieces) for place in down_places]).astype(jnp.int32)

    def down_of(k, *hidden):
        part = jax.ShapeDtypeStruct((each * pieces, rows, deep), bf16)
        return call(
            functools.partial(down_kernel, each, pieces, k * each * pieces, tuple(p for _, p in hidden)),
            local_places, *(h for h, _ in hidden), *downs[k * each : (k + 1) * each],
            out_shape=(part,) * len(hidden),
            in_specs=[SMEM] + [VMEM] * len(hidden) + [HBM] * each,
            out_specs=(VMEM,) * len(hidden),
            scratch_shapes=[
                pltpu.VMEM((each, units, deep * pieces), bf16),
                pltpu.VMEM((len(hidden) * rows, units), bf16),
                pltpu.SemaphoreType.DMA((each,)),
            ],
            compiler_params=params(20),
            cost_estimate=cost(2 * len(hidden) * rows * model * units // n_g, 6e6 // n_g),
        )

    opened = hidden_of((1, 0), (0,))
    hidden = [hidden_of((1, 0), (1,), (opened,))] + [hidden_of((s,)) for s in range(2, n_f)]
    sums = []
    for k in range(n_g):
        late = k > 0 and n_f > 3
        if late:
            total, second = down_of(k, (hidden[0], 0), (hidden[1], 0))
        else:
            (total,) = down_of(k, (hidden[0], 0))
        for s in range(2, n_f):
            more = [(hidden[s - 1], 0)] + ([(hidden[0], 1)] if s == n_f - 1 else [])
            added, *own = (second,) if late and s == 2 else down_of(k, *more)
            total = (ring(total).astype(f32) + added.astype(f32)).astype(bf16)
        sums += [own[0], ring(total)]
    (out,) = once(
        functools.partial(last_kernel, n_g, each * pieces, pieces),
        (g[None].astype(jnp.int32),),
        (middle, *sums),
        (jax.ShapeDtypeStruct((rows, model), bf16),),
    )
    return out


def solution(mesh):
    sizes = (mesh.shape["sp"], mesh.shape["tp"])
    in_specs = (
        P(AXES, None),
        P("sp", "tp"), P("sp", "tp"), P("sp", "tp"), P("sp", "tp"),
        P("sp", None, None),
        P("sp", "tp"), P("sp", "tp"), P("sp", "tp"), P("sp", "tp"),
        P("tp"), P("tp"),
        P(None, "tp"), P(None, "tp"),
        P(),
        P("tp"), P("tp"),
        P("tp", None), P("tp", None),
        P(),
        P("sp", "tp"), P("sp", "tp"), P("tp", "sp"),
    )

    def layer(*args):
        return on_device(sizes, *args)

    return jax.shard_map(layer, mesh=mesh, in_specs=in_specs, out_specs=P(AXES, None), check_vma=False)
```

```python
import functools

import jax
import jax.numpy as jnp
from jax import lax
from jax.experimental import pallas as pl
from jax.experimental.pallas import tpu as pltpu
from jax.sharding import PartitionSpec as P


HIGH = lax.Precision.HIGHEST
HEAD_EPS = 1e-05
ROW_EPS = 1e-06
HALO = 8
EXTRA = 16
AXES = ("sp", "tp")


f32 = jnp.float32
bf16 = jnp.bfloat16
VMEM = pl.BlockSpec(memory_space=pltpu.VMEM)
SMEM = pl.BlockSpec(memory_space=pltpu.SMEM)
HBM = pl.BlockSpec(memory_space=pltpu.HBM)
ANY = pl.BlockSpec(memory_space=pl.ANY)


def block_of(length):
    for size in (128, 64, 32, 16, 8):
        if length % size == 0:
            return size
    return length


def dot(a, b, precision=None):
    return jnp.dot(a, b, preferred_element_type=f32, precision=precision)


def dot_first(a, b, precision=None):
    return lax.dot_general(a, b, (((0,), (0,)), ((), ())), preferred_element_type=f32, precision=precision)


def dot_last(a, b, precision=None):
    return lax.dot_general(a, b, (((1,), (1,)), ((), ())), preferred_element_type=f32, precision=precision)


def one_hot(heads, widths, mean=False):
    count = padded(sum(heads))
    total = sum(widths)
    head = lax.broadcasted_iota(jnp.int32, (count, total), 0)
    channel = lax.broadcasted_iota(jnp.int32, (count, total), 1)
    hot = jnp.zeros((count, total), f32)
    first, start = 0, 0
    for number, width in zip(heads, widths):
        size = width // number
        low = start + (head - first) * size
        inside = (head >= first) & (head < first + number) & (channel >= low) & (channel < low + size)
        hot = jnp.where(inside, 1.0 / size if mean else 1.0, hot)
        first += number
        start += width
    return hot


def padded(count):
    return -(-count // 8) * 8


def silu(x):
    return x * (1.0 / (1.0 + jnp.exp(-x)))


def conv(pad_ref, halo, series, taps):
    length, width = series.shape
    pad_ref[0:HALO, 0:width] = halo.astype(f32)
    pad_ref[HALO : HALO + length, 0:width] = series.astype(f32)
    total = jnp.zeros((length, width), f32)
    for k, tap in enumerate(taps):
        first = HALO - (len(taps) - 1) + k
        total = total + tap.astype(f32) * pad_ref[first : first + length, 0:width]
    return silu(total)


def softplus(x):
    return jnp.maximum(x, 0.0) + jnp.log1p(jnp.exp(-jnp.abs(x)))


def edge_kernel(state, vs_ref, vl_ref, proj_ref, out_ref):
    first = vs_ref.shape[1]
    second = first + vl_ref.shape[1]
    out_ref[:, :first] = vs_ref[...]
    out_ref[:, first:second] = vl_ref[...]
    for plane in range(proj_ref.shape[1]):
        lo = second + plane * state
        out_ref[:, lo : lo + state] = proj_ref[:, plane, :]


def start_kernel(widths, heads, state, rs_ref, rl_ref, halo_ref, vs_ref, vl_ref, proj_ref, ss_ref, sl_ref, os_ref, ol_ref,
                 ts_ref, tl_ref, tm_ref, driven_ref, maps_ref, cum_ref, msg_ref, pad_ref, step_ref):
    length = vs_ref.shape[0]
    size = block_of(length)
    step_ref[...] = jnp.zeros_like(step_ref)
    cum_ref[...] = jnp.zeros_like(cum_ref)
    first = 0
    for number, s_ref, o_ref, r_ref in ((heads[0], ss_ref, os_ref, rs_ref), (heads[1], sl_ref, ol_ref, rl_ref)):
        step = softplus(s_ref[...].astype(f32))
        step_ref[first : first + number, :] = step
        for h in range(number):
            rate = jnp.exp(jnp.full((1, length), r_ref[h], f32))
            cum_ref[first + h : first + h + 1, :] = o_ref[h : h + 1, :] - rate * step[h : h + 1, :]
        first += number
    row = lax.broadcasted_iota(jnp.int32, (size, size), 0)
    col = lax.broadcasted_iota(jnp.int32, (size, size), 1)
    tri = jnp.where(row <= col, 1.0, 0.0).astype(f32)
    base = jnp.zeros((cum_ref.shape[0], 1), f32)
    for i in range(length // size):
        within = dot(cum_ref[:, i * size : (i + 1) * size], tri, HIGH) + base
        cum_ref[:, i * size : (i + 1) * size] = within
        base = within[:, size - 1 : size]
    hot = one_hot(heads, widths)
    count = tm_ref.shape[0]
    for plane in range(4):
        lo = plane * state
        at = sum(widths) + lo
        taps = [tm_ref[k, plane : plane + 1, :] for k in range(count)]
        done = conv(pad_ref, halo_ref[:, at : at + state], proj_ref[:, plane, :], taps)
        maps_ref[:, lo : lo + state] = done.astype(bf16)
    steps = dot_first(step_ref[...], hot, HIGH)
    tails = dot_first(jnp.exp(base - cum_ref[...]), hot, HIGH)
    offset = 0
    for kind, (width, v_ref, t_ref) in enumerate(((widths[0], vs_ref, ts_ref), (widths[1], vl_ref, tl_ref))):
        there = slice(offset, offset + width)
        taps = [t_ref[k : k + 1, :] for k in range(count)]
        driven = conv(pad_ref, halo_ref[:, there], v_ref[...], taps) * steps[:, there]
        driven_ref[:, there] = driven.astype(bf16)
        keys = maps_ref[:, 2 * kind * state : (2 * kind + 1) * state]
        msg_ref[0:state, there] = dot_first(keys, (driven * tails[:, there]).astype(bf16)).astype(bf16)
        offset += width
    write_decay(msg_ref, state, dot_first(jnp.exp(base), hot, HIGH))


def write_decay(ref, state, decay):
    high = decay.astype(bf16).astype(f32)
    index = lax.broadcasted_iota(jnp.int32, (EXTRA, decay.shape[1]), 0)
    rows = jnp.where(index == 0, high, jnp.where(index == 1, decay - high, 0.0))
    ref[state : state + EXTRA, :] = rows.astype(bf16)


def decay_of(ref, state):
    return ref[state : state + 1, :].astype(f32) + ref[state + 1 : state + 2, :].astype(f32)


def local_kernel(widths, heads, state, driven_ref, maps_ref, cum_ref, out_ref):
    length = driven_ref.shape[0]
    size = block_of(length)
    row = lax.broadcasted_iota(jnp.int32, (size, size), 0)
    col = lax.broadcasted_iota(jnp.int32, (size, size), 1)
    mask = row >= col
    hot = one_hot(heads, widths)
    base = jnp.zeros((cum_ref.shape[0], 1), f32)
    carry = [jnp.zeros((state, width), f32) for width in widths]
    for i in range(length // size):
        here = slice(i * size, (i + 1) * size)
        within = cum_ref[:, here] - base
        down = within.T
        last = within[:, size - 1 : size]
        grown = dot_first(jnp.exp(within), hot, HIGH)
        tails = dot_first(jnp.exp(last - within), hot, HIGH)
        whole = grown[size - 1 : size, :]
        base = base + last
        offset, first = 0, 0
        for kind in range(2):
            width, number = widths[kind], heads[kind]
            each = width // number
            there = slice(offset, offset + width)
            keys = maps_ref[here, 2 * kind * state : (2 * kind + 1) * state]
            reads = maps_ref[here, (2 * kind + 1) * state : (2 * kind + 2) * state]
            driven = driven_ref[here, there]
            scores = dot_last(reads, keys)
            parts = []
            for h in range(number):
                gap = down[:, first + h : first + h + 1] - within[first + h : first + h + 1, :]
                weights = jnp.where(mask, jnp.exp(jnp.where(mask, gap, 0.0)), 0.0)
                parts.append(dot((scores * weights).astype(bf16), driven[:, h * each : (h + 1) * each]))
            inner = jnp.concatenate(parts, axis=1) if number > 1 else parts[0]
            if i > 0:
                inner = inner + dot(reads, carry[kind].astype(bf16)) * grown[:, there]
            out_ref[here, there] = inner
            if i + 1 < length // size:
                fresh = (driven.astype(f32) * tails[:, there]).astype(bf16)
                carry[kind] = carry[kind] * whole[:, there] + dot_first(keys, fresh)
            offset += width
            first += number


def group_kernel(group, state, place_ref, *refs):
    out_ref, before_ref = refs[group], refs[group + 1]
    place = place_ref[0]
    places = [lax.rem(place - k + group, group) for k in range(group)]
    decays = [decay_of(ref, state) for ref in refs[:group]]
    ones = jnp.ones_like(decays[0])
    total = jnp.zeros((state, ones.shape[1]), f32)
    before = jnp.zeros_like(total)
    total_decay = ones
    before_decay = ones
    for k in range(group):
        rest = ones
        rest_before = ones
        for m in range(group):
            if m != k:
                rest = jnp.where(places[m] > places[k], rest * decays[m], rest)
                rest_before = jnp.where((places[m] > places[k]) & (places[m] < place), rest_before * decays[m], rest_before)
        values = refs[k][0:state, :].astype(f32)
        total = total + values * rest
        total_decay = total_decay * decays[k]
        if k > 0:
            is_before = places[k] < place
            before = before + jnp.where(is_before, values * rest_before, 0.0)
            before_decay = jnp.where(is_before, before_decay * decays[k], before_decay)
    for ref, values, decay in ((out_ref, total, total_decay), (before_ref, before, before_decay)):
        ref[0:state, :] = values.astype(bf16)
        write_decay(ref, state, decay)


def finish_kernel(widths, heads, state, ways, hops, place_ref, gs_far, gl_far, ws_far, wl_far, local_ref, maps_ref, cum_ref,
                  hs_ref, hl_ref, before_ref, *refs):
    arrived = refs[:hops]
    keep_ref, send_ref, rows_ref, gs_ref, gl_ref, ws_ref, wl_ref, sems = refs[hops:]
    pairs = ((gs_far, gs_ref), (gl_far, gl_ref), (ws_far, ws_ref), (wl_far, wl_ref))
    copies = [pltpu.make_async_copy(far, near, sems.at[k]) for k, (far, near) in enumerate(pairs)]
    for copy in copies:
        copy.start()
    length = local_ref.shape[0]
    size = block_of(length)
    incoming = jnp.zeros((state, local_ref.shape[1]), f32)
    for ref in reversed(arrived):
        incoming = ref[0:state, :].astype(f32) + decay_of(ref, state) * incoming
    incoming = incoming * decay_of(before_ref, state) + before_ref[0:state, :].astype(f32)
    incoming = incoming.astype(bf16)
    hot = one_hot(heads, widths)
    hot_mean = one_hot(heads, widths, mean=True)
    copies[0].wait()
    copies[1].wait()
    for i in range(length // size):
        here = slice(i * size, (i + 1) * size)
        grown = dot_first(jnp.exp(cum_ref[:, here]), hot, HIGH)
        parts = []
        offset = 0
        for kind, g_ref in enumerate((gs_ref, gl_ref)):
            there = slice(offset, offset + widths[kind])
            reads = maps_ref[here, (2 * kind + 1) * state : (2 * kind + 2) * state]
            scan = local_ref[here, there] + dot(reads, incoming[:, there]) * grown[:, there]
            parts.append(scan * silu(g_ref[here, :].astype(f32)))
            offset += widths[kind]
        squares = jnp.concatenate([part * part for part in parts], axis=1)
        scale = dot(lax.rsqrt(dot_last(squares, hot_mean, HIGH) + HEAD_EPS), hot, HIGH)
        offset = 0
        for part, h_ref in zip(parts, (hs_ref, hl_ref)):
            there = slice(offset, offset + part.shape[1])
            rows_ref[here, there] = (part * scale[:, there] * h_ref[...]).astype(bf16)
            offset += part.shape[1]
    place = place_ref[0]
    per = length // ways
    copies[2].wait()
    copies[3].wait()
    for slot in range(ways // 2):
        for bit, ref in ((1, send_ref), (0, keep_ref)):
            start = pl.multiple_of(jnp.bitwise_xor(place, 2 * slot + bit) * per, per)
            rows = rows_ref[pl.ds(start, per), :]
            part = dot(rows[:, : widths[0]], ws_ref[...]) + dot(rows[:, widths[0] :], wl_ref[...])
            ref[slot] = part.astype(bf16)


def norm_kernel(blocks, residual_ref, own_ref, other_ref, gain_ref, middle_ref, normed_ref):
    middle = residual_ref[...].astype(f32) + (own_ref[...].astype(f32) + other_ref[...].astype(f32))
    middle = middle.astype(bf16)
    middle_ref[...] = middle
    wide = middle.astype(f32)
    scale = lax.rsqrt(jnp.mean(wide * wide, axis=-1, keepdims=True) + ROW_EPS)
    normed = (wide * scale * gain_ref[...]).astype(bf16)
    width = normed.shape[1] // blocks
    for b in range(blocks):
        normed_ref[b] = normed[:, b * width : (b + 1) * width]


def join_kernel(axis, first_ref, second_ref, out_ref, sems):
    copies = []
    for k, ref in enumerate((first_ref, second_ref)):
        there = pl.ds(k * ref.shape[axis], ref.shape[axis])
        target = out_ref.at[there, :] if axis == 0 else out_ref.at[:, there]
        copies.append(pltpu.make_async_copy(ref, target, sems.at[k]))
    for copy in copies:
        copy.start()
    for copy in copies:
        copy.wait()


def cut_kernel(axis, part, block_ref, out_ref, sems):
    there = pl.ds(part * out_ref.shape[axis], out_ref.shape[axis])
    copy = pltpu.make_async_copy(block_ref.at[there, :] if axis == 0 else block_ref.at[:, there], out_ref, sems.at[0])
    copy.start()
    copy.wait()


def last_kernel(group, count, pieces, place_ref, middle_ref, *refs):
    out_ref = refs[2 * group]
    deep = refs[0].shape[2]
    for k in range(group):
        own_ref, other_ref = refs[2 * k], refs[2 * k + 1]
        part = lax.rem(place_ref[0] - k + group, group)
        for b in range(count):
            first, second = b // pieces * group * pieces, b % pieces
            start = (first + part * pieces + second) * deep
            there = pl.ds(pl.multiple_of(start, deep), deep)
            added = own_ref[b].astype(f32) + other_ref[b].astype(f32)
            out_ref[:, there] = (middle_ref[:, there].astype(f32) + added).astype(bf16)


def hidden_kernel(blocks, pieces, kinds, index_ref, *refs):
    out_ref, weight_ref, cat_ref, part_ref, chunks_ref, sems = refs[-6:]
    inputs = refs[:-6]
    weights = inputs[len(inputs) - len(kinds) * blocks :]
    far = inputs[: len(inputs) - len(kinds) * blocks]
    rows, deep = chunks_ref.shape[2:]
    depth = deep * pieces
    units = out_ref.shape[1]
    tile = 256
    cut = units // (2 * tile) * tile
    spans = ((0, cut), (cut, units)) if cut else ((0, units),)
    arrivals = []
    if kinds == (1,):
        arrivals.append(pltpu.make_async_copy(far[-1], part_ref, sems.at[2, 0, blocks - 1]))
        far = far[:-1]
    arrivals += [pltpu.make_async_copy(ref, chunks_ref.at[j], sems.at[2, 0, j]) for j, ref in enumerate(far)]
    copies = []
    for n in range(len(kinds)):
        for p, (low, high) in enumerate(spans):
            for b in range(blocks):
                source = weights[n * blocks + b].at[:, low:high]
                target = weight_ref.at[n, pl.ds(b * depth, depth), low:high]
                copies.append(pltpu.make_async_copy(source, target, sems.at[n, p, b]))
    for copy in arrivals + copies:
        copy.start()
    for copy in arrivals:
        copy.wait()
    for n, kind in enumerate(kinds):
        for k in range(blocks * pieces):
            place = index_ref[kind * blocks * pieces + k]
            for j in range(len(far)):
                cat_ref[n, j * rows : (j + 1) * rows, k * deep : (k + 1) * deep] = chunks_ref[j, place]

        def some(here, n=n, kind=kind):
            value = dot(cat_ref[n], weight_ref[n, :, here])
            if kind == 1:
                out_ref[:, here] = (part_ref[:, here] * value).astype(bf16)
            elif len(kinds) == 2:
                part_ref[:, here] = silu(value)
            else:
                out_ref[:, here] = silu(value)

        def one(i, _, some=some):
            some(pl.ds(pl.multiple_of(i * tile, tile), tile))
            return 0

        for p, (low, high) in enumerate(spans):
            for copy in copies[(n * len(spans) + p) * blocks : (n * len(spans) + p + 1) * blocks]:
                copy.wait()
            lax.fori_loop(low // tile, high // tile, one, 0)
            if high % tile:
                some(slice(high // tile * tile, high))


def down_kernel(blocks, pieces, start, parts, index_ref, *refs):
    hidden = refs[: len(parts)]
    weights = refs[len(parts) : len(parts) + blocks]
    outs = refs[len(parts) + blocks : 2 * len(parts) + blocks]
    down_ref, cat_ref, sems = refs[-3:]
    rows, deep = outs[0].shape[1:]
    copies = [pltpu.make_async_copy(weights[b], down_ref.at[b], sems.at[b]) for b in range(blocks)]
    for copy in copies:
        copy.start()
    for j, part in enumerate(parts):
        cat_ref[j * rows : (j + 1) * rows, :] = hidden[j][part * rows : (part + 1) * rows, :]
    for b in range(blocks):
        copies[b].wait()
        out = dot(cat_ref[...], down_ref[b]).astype(bf16)
        for k in range(pieces):
            place = index_ref[start + b * pieces + k]
            for j, ref in enumerate(outs):
                ref[place] = out[j * rows : (j + 1) * rows, k * deep : (k + 1) * deep]


def full(*arrays):
    return [pl.BlockSpec(a.shape, functools.partial(lambda n, i: (0,) * n, len(a.shape))) for a in arrays]


def params(mib):
    return pltpu.CompilerParams(vmem_limit_bytes=mib * 1024 * 1024)


def cost(flops, nbytes):
    return pl.CostEstimate(flops=int(flops), bytes_accessed=int(nbytes), transcendentals=0)


def on_device(sizes, residual, small_values, large_values, small_gates, large_gates, state_projections, small_steps, large_steps,
              small_offsets, large_offsets, small_rates, large_rates, small_taps, large_taps, state_taps, small_gains, large_gains,
              small_projection, large_projection, norm_gain, gate_matrix, up_matrix, down_matrix):
    n_sp, n_tp = sizes
    n_f = n_tp
    n_g = n_sp // n_f
    n_x = n_tp // 2
    sp = lax.axis_index("sp")
    tp = lax.axis_index("tp")
    g = lax.rem(sp, n_g)

    def send(x, to):
        pairs = []
        for s in range(n_sp):
            for t in range(n_tp):
                target = to(s // n_g, s % n_g, t)
                if target is not None:
                    pairs.append((s * n_tp + t, (target[0] * n_g + target[1]) * n_tp + target[2]))
        return lax.ppermute(x, AXES, pairs)

    def call(kernel, *args, **kw):
        return pl.pallas_call(kernel, **kw)(*args)

    def once(kernel, scalars, args, outs, scratch=(), mib=24, flops=4e9, far=()):
        return call(
            kernel,
            *scalars,
            *far,
            *args,
            grid=(1,),
            out_shape=tuple(outs),
            in_specs=[SMEM] * len(scalars) + [HBM] * len(far) + full(*args),
            out_specs=tuple(full(*outs)),
            scratch_shapes=list(scratch),
            compiler_params=params(mib),
            cost_estimate=cost(flops, 4e6),
        )

    length, width_small = small_values.shape
    width_large = large_values.shape[1]
    widths = (width_small, width_large)
    width = width_small + width_large
    heads = (small_rates.shape[0], large_rates.shape[0])
    planes, state = state_projections.shape[1:]
    rows, model = residual.shape

    last = length // HALO - 1
    edge = call(
        functools.partial(edge_kernel, state),
        small_values, large_values, state_projections,
        grid=(1,),
        out_shape=jax.ShapeDtypeStruct((HALO, width + planes * state), bf16),
        in_specs=[
            pl.BlockSpec((HALO, width_small), lambda i: (last, 0)),
            pl.BlockSpec((HALO, width_large), lambda i: (last, 0)),
            pl.BlockSpec((HALO, planes, state), lambda i: (last, 0, 0)),
        ],
        out_specs=pl.BlockSpec((HALO, width + planes * state), lambda i: (0, 0)),
    )
    halo = lax.ppermute(edge, "sp", [(i, i + 1) for i in range(n_sp - 1)])

    f = sp // n_g
    x = tp // 2
    c = lax.rem(tp, 2)
    pieces = 2 if n_x == 2 else 1
    blocks = n_sp
    deep = model // (blocks * pieces)

    def plane_of(x_, c_):
        return x_ + n_x * c_

    def slot_of(f_, plane, x_):
        if n_x != 2:
            return f_ % n_x, f_ // n_x
        k = f_ ^ plane
        return (x_ ^ 1 if k < 2 else x_), k % 2

    def moved(matrix, axis, split):
        if not split:

            def to(f_, g_, t_):
                plane = plane_of(t_ // 2, t_ % 2)
                x_, c_ = slot_of(f_, plane, t_ // 2)
                return plane, g_, 2 * x_ + c_

            return send(matrix, to)
        first = lax.slice_in_dim(matrix, 0, deep, axis=axis)
        second = lax.slice_in_dim(matrix, deep, 2 * deep, axis=axis)
        second = send(second, lambda f_, g_, t_: (f_, g_, t_ ^ 2))
        even = lax.rem(f, 2) == 0
        got = []
        for k, out in enumerate((jnp.where(even, first, second), jnp.where(even, second, first))):

            def to(f_, g_, t_, k=k):
                x_, c_ = t_ // 2, t_ % 2
                own = (f_ % 2 == 0) == (k == 0)
                return plane_of(x_ if own else 1 - x_, c_), g_, 2 * x_ + f_ // 2

            got.append(send(out, to))
        return joined_of(axis, *got)

    def joined_of(axis, *parts):
        shape = tuple(2 * deep if i == axis else n for i, n in enumerate(parts[0].shape))
        return call(
            functools.partial(join_kernel, axis),
            *parts,
            out_shape=jax.ShapeDtypeStruct(shape, bf16),
            in_specs=[HBM] * 2,
            out_specs=HBM,
            scratch_shapes=[pltpu.SemaphoreType.DMA((2,))],
            compiler_params=params(4),
            cost_estimate=cost(1e6, 3e6),
        )

    def cut_of(axis, part, block):
        shape = tuple(deep if i == axis else n for i, n in enumerate(block.shape))
        return call(
            functools.partial(cut_kernel, axis, part),
            block,
            out_shape=jax.ShapeDtypeStruct(shape, bf16),
            in_specs=[HBM],
            out_specs=HBM,
            scratch_shapes=[pltpu.SemaphoreType.DMA((1,))],
            compiler_params=params(4),
            cost_estimate=cost(1e6, 1e6),
        )

    def gathered(matrix, axis, order, split, both=False):
        held = [(moved(matrix, axis, split), (0, 0, 0))]
        if both:
            def over_x(block):
                return send(block, lambda f_, g_, t_: (f_, g_, t_ ^ 2))

            def over_g(block):
                return send(block, lambda f_, g_, t_: (f_, 1 - g_, t_))

            own = held[0][0]
            one, other = over_x(own), over_g(own)
            second = over_x(cut_of(axis, 1, other))
            first = over_g(cut_of(axis, 0, one))
            held += [(one, (1, 0, 0)), (other, (0, 1, 0)), (joined_of(axis, first, second), (1, 1, 0))]
            order = (2,)
        for kind in order:
            count = (n_x, n_g, 2)[kind]
            new = []
            for k in range(1, count):
                for block, way in held:
                    if kind == 0:
                        got = send(block, lambda f_, g_, t_: (f_, g_, 2 * ((t_ // 2 + k) % n_x) + t_ % 2))
                    elif kind == 1:
                        got = send(block, lambda f_, g_, t_: (f_, (g_ + k) % n_g, t_))
                    else:
                        got = send(block, lambda f_, g_, t_: (f_, g_, t_ ^ 1))
                    moved_by = list(way)
                    moved_by[kind] += k
                    new.append((got, tuple(moved_by)))
            held = held + new
        held.sort(key=lambda item: item[1][1])
        places = []
        for _, (dx, dg, dc) in held:
            x_ = lax.rem(x - dx + n_x, n_x)
            c_ = lax.rem(c - dc + 2, 2)
            g_ = lax.rem(g - dg + n_g, n_g)
            if split:
                own = lax.rem(f, 2) == x_
                for k in range(2):
                    f_ = 2 * c_ + jnp.where(own, k, 1 - k)
                    places.append((f_ * n_g + g_) * 2 + jnp.where(own, 0, 1))
                continue
            if n_x == 2:
                crossed = lax.rem(f, 2) != x_
                f_ = jnp.bitwise_xor(f, jnp.where(crossed, c_, 2 + c_))
            else:
                f_ = c_ * n_x + x_
            places += [(f_ * n_g + g_) * pieces + k for k in range(pieces)]
        return [block for block, _ in held], places

    two = n_x == 2
    gates, gate_places = gathered(gate_matrix, 0, (0, 1, 2), False)
    ups, up_places = gathered(up_matrix, 0, (0, 1, 2), two, two and n_g == 2)
    downs, down_places = gathered(down_matrix, 1, (0, 1, 2), two)
    index = jnp.stack(gate_places + up_places + down_places).astype(jnp.int32)

    message = jax.ShapeDtypeStruct((state + EXTRA, width), bf16)
    per_head = (padded(sum(heads)), length)
    driven, maps, cum, own = once(
        functools.partial(start_kernel, widths, heads, state),
        (small_rates, large_rates),
        (halo, small_values, large_values, state_projections, small_steps.T, large_steps.T, small_offsets.T, large_offsets.T,
         small_taps, large_taps, state_taps),
        (
            jax.ShapeDtypeStruct((length, width), bf16),
            jax.ShapeDtypeStruct((length, planes * state), bf16),
            jax.ShapeDtypeStruct(per_head, f32),
            message,
        ),
        (pltpu.VMEM((HALO + length, max(widths + (state,))), f32), pltpu.VMEM(per_head, f32)),
    )
    others = [send(own, lambda f_, g_, t_: (f_, (g_ + k) % n_g, t_)) for k in range(1, n_g)]
    (local,) = once(
        functools.partial(local_kernel, widths, heads, state),
        (),
        (driven, maps, cum),
        (jax.ShapeDtypeStruct((length, width), f32),),
    )
    joined, before = once(
        functools.partial(group_kernel, n_g, state), (g[None].astype(jnp.int32),), (own, *others), (message, message)
    )
    arrived = [send(joined, lambda f_, g_, t_: (f_ + k, g_, t_) if f_ + k < n_f else None) for k in range(1, n_f)]

    half = n_tp // 2
    part = jax.ShapeDtypeStruct((half, rows, model), bf16)
    keep, give = once(
        functools.partial(finish_kernel, widths, heads, state, n_tp, len(arrived)),
        (tp[None].astype(jnp.int32),),
        (local, maps, cum, small_gains[None, :], large_gains[None, :], before, *arrived),
        (part, part),
        (
            pltpu.VMEM((length, width), bf16),
            pltpu.VMEM(small_gates.shape, bf16),
            pltpu.VMEM(large_gates.shape, bf16),
            pltpu.VMEM(small_projection.shape, bf16),
            pltpu.VMEM(large_projection.shape, bf16),
            pltpu.SemaphoreType.DMA((4,)),
        ),
        mib=32,
        far=(small_gates, large_gates, small_projection, large_projection),
    )

    got = send(give, lambda f_, g_, t_: (f_, g_, t_ ^ 1))
    kept = [keep[i] for i in range(half)]
    arriving = [got[i] for i in range(half)]
    bit = 2
    while len(kept) > 1:
        sent = []
        stay = []
        for i in range(0, len(kept), 2):
            stay.append((kept[i].astype(f32) + arriving[i].astype(f32)).astype(bf16))
            sent.append((kept[i + 1].astype(f32) + arriving[i + 1].astype(f32)).astype(bf16))
        arriving = [send(x, lambda f_, g_, t_, b=bit: (f_, g_, t_ ^ b)) for x in sent]
        kept = stay
        bit *= 2
    chunk_shape = jax.ShapeDtypeStruct((blocks * pieces, rows, deep), bf16)
    middle, normed = once(
        functools.partial(norm_kernel, blocks * pieces),
        (),
        (residual, kept[0], arriving[0], norm_gain[None, :]),
        (jax.ShapeDtypeStruct((rows, model), bf16), chunk_shape),
    )

    units = gate_matrix.shape[1]
    each = blocks // n_g

    def ring(x):
        return send(x, lambda f_, g_, t_: ((f_ + 1) % n_f, g_, t_))

    chunks = [normed]
    for _ in range(1, n_f):
        chunks.append(ring(chunks[-1]))

    def hidden_of(which, kinds=(0, 1), first=()):
        count = len(which) * rows
        weights = [block for kind in kinds for block in (gates, ups)[kind]]
        return call(
            functools.partial(hidden_kernel, blocks, pieces, kinds),
            index, *(chunks[s] for s in which), *first, *weights,
            out_shape=jax.ShapeDtypeStruct((count, units), f32 if kinds == (0,) else bf16),
            in_specs=[SMEM] + [ANY] * (len(which) + len(first)) + [HBM] * len(weights),
            out_specs=VMEM,
            scratch_shapes=[
                pltpu.VMEM((len(kinds), model, units), bf16),
                pltpu.VMEM((len(kinds), count, model), bf16),
                pltpu.VMEM((count, units), f32),
                pltpu.VMEM((len(which), blocks * pieces, rows, deep), bf16),
                pltpu.SemaphoreType.DMA((3, 2, blocks)),
            ],
            compiler_params=params(28 if len(kinds) == 2 else 56),
            cost_estimate=cost(2 * len(kinds) * count * model * units, 6e6 * len(kinds)),
        )

    local_places = jnp.stack([place // (n_g * pieces) * pieces + lax.rem(place, pieces) for place in down_places]).astype(jnp.int32)

    def down_of(k, *hidden):
        part = jax.ShapeDtypeStruct((each * pieces, rows, deep), bf16)
        return call(
            functools.partial(down_kernel, each, pieces, k * each * pieces, tuple(p for _, p in hidden)),
            local_places, *(h for h, _ in hidden), *downs[k * each : (k + 1) * each],
            out_shape=(part,) * len(hidden),
            in_specs=[SMEM] + [VMEM] * len(hidden) + [HBM] * each,
            out_specs=(VMEM,) * len(hidden),
            scratch_shapes=[
                pltpu.VMEM((each, units, deep * pieces), bf16),
                pltpu.VMEM((len(hidden) * rows, units), bf16),
                pltpu.SemaphoreType.DMA((each,)),
            ],
            compiler_params=params(20),
            cost_estimate=cost(2 * len(hidden) * rows * model * units // n_g, 6e6 // n_g),
        )

    opened = hidden_of((1, 0), (0,))
    hidden = [hidden_of((1, 0), (1,), (opened,))] + [hidden_of((s,)) for s in range(2, n_f)]
    sums = []
    for k in range(n_g):
        late = k > 0 and n_f > 3
        if late:
            total, second = down_of(k, (hidden[0], 0), (hidden[1], 0))
        else:
            (total,) = down_of(k, (hidden[0], 0))
        for s in range(2, n_f):
            more = [(hidden[s - 1], 0)] + ([(hidden[0], 1)] if s == n_f - 1 else [])
            added, *own = (second,) if late and s == 2 else down_of(k, *more)
            total = (ring(total).astype(f32) + added.astype(f32)).astype(bf16)
        sums += [own[0], ring(total)]
    (out,) = once(
        functools.partial(last_kernel, n_g, each * pieces, pieces),
        (g[None].astype(jnp.int32),),
        (middle, *sums),
        (jax.ShapeDtypeStruct((rows, model), bf16),),
    )
    return out


def solution(mesh):
    sizes = (mesh.shape["sp"], mesh.shape["tp"])
    in_specs = (
        P(AXES, None),
        P("sp", "tp"), P("sp", "tp"), P("sp", "tp"), P("sp", "tp"),
        P("sp", None, None),
        P("sp", "tp"), P("sp", "tp"), P("sp", "tp"), P("sp", "tp"),
        P("tp"), P("tp"),
        P(None, "tp"), P(None, "tp"),
        P(),
        P("tp"), P("tp"),
        P("tp", None), P("tp", None),
        P(),
        P("sp", "tp"), P("sp", "tp"), P("tp", "sp"),
    )

    def layer(*args):
        return on_device(sizes, *args)

    return jax.shard_map(layer, mesh=mesh, in_specs=in_specs, out_specs=P(AXES, None), check_vma=False)
```
